128 devices in a mesh: sp: 32 (over z, y, core), tp: 4 (over x).
Axes of the slice: x: 4, y: 4, z: 4, core: 2. Of those that a mesh axis runs over, the one named last changes fastest.
Arguments:
- tokens: bfloat16 [8192, 4096], P(('sp', 'tp')), may hold values from -6 to 6, as said below
- query_one: bfloat16 [4096, 1024], P('sp', 'tp'), may hold values from -0.125 to 0.125
- query_two: bfloat16 [4096, 1024], P('sp', 'tp'), may hold values from -0.125 to 0.125
- key_one: bfloat16 [4096, 1024], P('sp', 'tp'), may hold values from -0.125 to 0.125
- key_two: bfloat16 [4096, 1024], P('sp', 'tp'), may hold values from -0.125 to 0.125
- value_weight: bfloat16 [4096, 2048], P('sp', 'tp'), may hold values from -0.09375 to 0.09375
- out_weight: bfloat16 [2048, 4096], P('tp', 'sp'), may hold values from -0.125 to 0.125
- lambdas: float32 [8], P('tp'), may hold values from 0.3 to 0.8
- head_gain: float32 [256], replicated, may hold values from 0.1 to 1.9
Outputs:
- layer_out: bfloat16 [8192, 4096], P(('sp', 'tp'))
The draws below stay inside these ranges and needn't reach their ends.
Inputs may be any that keep to these rules, and one draw needn't show every extreme that they name: `tokens`: the features' mean changes between 16 equal spans of the sequence.
All inputs are finite; a program needn't handle non-finite values.
Results may differ from the reference program's by a relative error of at most 0.013.
The reference program's roundings to bfloat16 on the way count: a program that leaves them out, or rounds other values in their place, can miss the bound.
Values may be sent and summed in bfloat16 or wider, within the bound.
A program may use at most 128 MiB of HBM per device.

```python
import jax
import jax.numpy as jnp
from jax import lax

D = 4096
H = 8
QK = 128
V = 256
TOK_DEV = 256
TOKENS = 8192


def draw_tokens(key, part):
    base_key, mean_key, row_key = jax.random.split(key, 3)
    span_ids = jnp.arange(TOKENS, dtype=jnp.int32) * 16 // TOKENS
    span_means = 0.6 * jnp.clip(jax.random.normal(mean_key, (16, D), jnp.float32), -2.5, 2.5)
    offsets = span_means[span_ids]
    base_draw = jnp.clip(jax.random.normal(base_key, (TOKENS, D), jnp.float32), -4.5, 4.5)
    values = jnp.clip(base_draw + offsets, -6.0, 6.0)
    return values.astype(jnp.bfloat16)


def block_scale(own_key, dims, cuts, smallest, high):
    gain = 1.0
    for dim, parts in cuts:
        heights = jax.random.uniform(jax.random.fold_in(jax.random.fold_in(own_key, 6), dim), (parts,), jnp.float32, smallest / len(cuts), high / len(cuts))
        gain = gain * jnp.repeat(jnp.exp(heights), dims[dim] // parts).reshape((-1,) + (1,) * (len(dims) - 1 - dim))
    return gain


def scatter_about(key, dims, scale, limit, cuts=(), held_as=jnp.bfloat16):
    values = jax.random.normal(key, dims, jnp.float32) * scale
    if len(cuts) > 0:
        values = block_scale(key, dims, cuts, -0.22, 0.18) * values
    return jnp.clip(values, min=-limit, max=limit).astype(held_as)


def setup_inputs(seed: int = 0) -> dict:
    keys = jax.random.split(jax.random.key(seed), 10)
    tokens = draw_tokens(jax.random.fold_in(keys[9], 71), 0)
    query_one = scatter_about(keys[1], (D, H * QK), (D * 4 // 7) ** -0.5, 0.125, ((0, 32), (1, 4)))
    query_two = scatter_about(keys[2], (D, H * QK), (D * 4 // 7) ** -0.5, 0.125, ((0, 32), (1, 4)))
    key_one = scatter_about(keys[3], (D, H * QK), (D * 4 // 7) ** -0.5, 0.125, ((0, 32), (1, 4)))
    key_two = scatter_about(keys[4], (D, H * QK), (D * 4 // 7) ** -0.5, 0.125, ((0, 32), (1, 4)))
    value_weight = scatter_about(keys[5], (D, H * V), D ** -0.5, 0.09375, ((0, 32), (1, 4)))
    out_weight = scatter_about(keys[6], (H * V, D), (H * V) ** -0.5, 0.125, ((0, 4), (1, 32)))
    lambdas = jnp.clip(0.3 + 0.5 * jax.random.uniform(keys[7], (H,), jnp.float32) ** block_scale(keys[7], (H,), ((0, 4),), -0.2, 0.2), 0.3, 0.8)
    head_gain = jnp.clip(1.0 + 0.18 * jax.random.normal(keys[8], (V,), jnp.float32), 0.1, 1.9)
    return dict(tokens=tokens, query_one=query_one, query_two=query_two, key_one=key_one, key_two=key_two, value_weight=value_weight, out_weight=out_weight, lambdas=lambdas, head_gain=head_gain)


ROPE_BASE = 500000.0
EPS_NORM = 0.02

def rotate(values, positions):
    half_dim = values.shape[-1] // 2
    inverse = 1.0 / ROPE_BASE ** (jnp.arange(0, 2 * half_dim, 2, dtype=jnp.float32) / (2 * half_dim))
    angles = positions.astype(jnp.float32)[:, None] * inverse[None, :]
    cos_part = jnp.cos(angles)[:, None, :]
    sin_part = jnp.sin(angles)[:, None, :]
    first_half = values[..., :half_dim]
    second_half = values[..., half_dim:]
    return jnp.concatenate([first_half * cos_part - second_half * sin_part, second_half * cos_part + first_half * sin_part], axis=-1)

def reference(tokens, query_one, query_two, key_one, key_two, value_weight, out_weight, lambdas, head_gain):
    seq_len = tokens.shape[0]
    positions = jnp.arange(seq_len, dtype=jnp.int32)

    def project(weight):
        product = jnp.dot(tokens, weight, preferred_element_type=jnp.float32)
        return rotate(product.reshape(seq_len, H, QK), positions).astype(jnp.bfloat16)
    q_one = project(query_one)
    q_two = project(query_two)
    k_one = project(key_one)
    k_two = project(key_two)
    values = jnp.dot(tokens, value_weight, preferred_element_type=jnp.float32).astype(jnp.bfloat16)
    values = values.reshape(seq_len, H, V).astype(jnp.float32)
    block_len = TOK_DEV
    n_blocks = seq_len // block_len

    def one_block(block_index):
        start_row = block_index * block_len
        q_pos = start_row + jnp.arange(block_len, dtype=jnp.int32)
        allowed = positions[None, :] <= q_pos[:, None]
        map_outs = []
        for q_all, k_all in ((q_one, k_one), (q_two, k_two)):
            q_blk = lax.dynamic_slice_in_dim(q_all, start_row, block_len, 0)
            scores = jnp.einsum('qhd,khd->hqk', q_blk.astype(jnp.float32), k_all.astype(jnp.float32)) * QK ** (-0.5)
            masked = jnp.where(allowed[None], scores, -1e+30)
            row_top = lax.optimization_barrier(jnp.max(masked, axis=-1, keepdims=True))
            exp_weights = jnp.where(allowed[None], jnp.exp(scores - row_top), 0.0)
            row_total = lax.optimization_barrier(jnp.sum(exp_weights, axis=-1))
            rounded = lax.optimization_barrier(exp_weights.astype(jnp.bfloat16))
            weighted = jnp.einsum('hqk,khv->hqv', rounded.astype(jnp.float32), values)
            map_outs.append(weighted / row_total[..., None])
        mixed_out = map_outs[0] - lambdas[:, None, None] * map_outs[1]
        scaled = mixed_out * lax.rsqrt(lax.optimization_barrier(jnp.mean(mixed_out * mixed_out, axis=-1, keepdims=True)) + EPS_NORM) * head_gain
        return jnp.transpose(scaled, (1, 0, 2)).reshape(block_len, H * V).astype(jnp.bfloat16)
    attended = lax.map(one_block, jnp.arange(n_blocks, dtype=jnp.int32)).reshape(seq_len, H * V)
    return jnp.dot(attended, out_weight, preferred_element_type=jnp.float32).astype(jnp.bfloat16)
```

```python
import functools

import jax
import jax.numpy as jnp
from jax import lax
from jax.experimental import pallas as pl
from jax.experimental.pallas import tpu as pltpu
from jax.sharding import Mesh, PartitionSpec as P

QK = 128
V = 256
ROPE_BASE = 500000.0
EPS_NORM = 0.02
ROWS = 512
LOG2E = 1.4426950408889634


def rope_tables(positions):
    half = QK // 2
    inverse = 1.0 / ROPE_BASE ** (jnp.arange(0, QK, 2, dtype=jnp.float32) / QK)
    angles = positions.astype(jnp.float32)[:, None] * inverse[None, :]
    c, s = jnp.cos(angles), jnp.sin(angles)
    return jnp.concatenate([c, c], axis=1), jnp.concatenate([-s, s], axis=1)


def turned(x, cos, sin):
    half = QK // 2
    swapped = jnp.concatenate([x[:, half:], x[:, :half]], axis=1)
    return (x * cos + swapped * sin).astype(jnp.bfloat16)


def flash_kernel(n_chips, q1_ref, q2_ref, k1_ref, k2_ref, v_ref, lam_ref, gain_ref, out_ref, acc, top, tot):
    chip = lax.axis_index("z") * 4 + lax.axis_index("y")
    scale = QK ** (-0.5)
    qs = (q1_ref, q2_ref)
    ks = (k1_ref, k2_ref)
    for a in range(2):
        top[a] = jnp.full((ROWS, 128), -1e30, jnp.float32)
        tot[a] = jnp.zeros((ROWS, 128), jnp.float32)
        acc[a] = jnp.zeros((ROWS, V), jnp.float32)

    def block(j, diagonal):
        start = pl.multiple_of(j * ROWS, ROWS)
        v = v_ref[pl.ds(start, ROWS), :]
        for a in range(2):
            s = lax.dot_general(
                qs[a][...], ks[a][pl.ds(start, ROWS), :], (((1,), (1,)), ((), ())),
                preferred_element_type=jnp.float32,
            ) * scale
            if diagonal:
                rows = lax.broadcasted_iota(jnp.int32, s.shape, 0)
                cols = lax.broadcasted_iota(jnp.int32, s.shape, 1)
                s = jnp.where(cols <= rows, s, -1e30)
            old = top[a][:, :1]
            new = jnp.maximum(old, jnp.max(s, axis=1, keepdims=True))
            e = jnp.exp(s - new)
            fade = jnp.exp(old - new)
            tot[a] = tot[a] * fade + jnp.sum(e, axis=1, keepdims=True)
            acc[a] = acc[a] * fade + lax.dot_general(
                e.astype(jnp.bfloat16), v, (((1,), (0,)), ((), ())),
                preferred_element_type=jnp.float32,
            )
            top[a] = jnp.broadcast_to(new, (ROWS, 128))

    block(chip, True)

    @pl.loop(0, chip)
    def _(j):
        block(j, False)

    o1 = acc[0] / tot[0][:, :1]
    o2 = acc[1] / tot[1][:, :1]
    mixed = o1 - lam_ref[0] * o2
    norm = lax.rsqrt(jnp.mean(mixed * mixed, axis=1, keepdims=True) + EPS_NORM)
    out_ref[...] = (mixed * norm * gain_ref[...]).astype(jnp.bfloat16)


def flash(q1, q2, k1, k2, v, lam, gain):
    vm = pl.BlockSpec(memory_space=pltpu.VMEM)
    return pl.pallas_call(
        functools.partial(flash_kernel, 16),
        out_shape=jax.ShapeDtypeStruct((ROWS, V), jnp.bfloat16),
        in_specs=[vm] * 5 + [pl.BlockSpec(memory_space=pltpu.SMEM), vm],
        out_specs=vm,
        scratch_shapes=[
            pltpu.VMEM((2, ROWS, V), jnp.float32),
            pltpu.VMEM((2, ROWS, 128), jnp.float32),
            pltpu.VMEM((2, ROWS, 128), jnp.float32),
        ],
        compiler_params=pltpu.CompilerParams(vmem_limit_bytes=60 * 1024 * 1024),
        cost_estimate=pl.CostEstimate(flops=6 * 10**9, bytes_accessed=10**7, transcendentals=10**7),
    )(q1, q2, k1, k2, v, lam, gain)


def on_device(tokens, query_one, query_two, key_one, key_two, value_weight, out_weight, lambdas, head_gain):
    core = lax.axis_index("core")
    chip = lax.axis_index("z") * 4 + lax.axis_index("y")
    rows = lax.all_gather(tokens, ("core", "x"), axis=0, tiled=True)
    by_head = [w.reshape(128, 2, -1) for w in (query_one, query_two, key_one, key_two, value_weight)]
    both = jnp.concatenate(by_head, axis=2)
    mine = lax.all_to_all(both, "core", split_axis=1, concat_axis=0, tiled=True).reshape(256, 768)
    weights = lax.all_gather(mine, ("z", "y"), axis=0, tiled=True)
    projected = jnp.dot(rows, weights, preferred_element_type=jnp.float32)
    cos, sin = rope_tables(chip * ROWS + jnp.arange(ROWS, dtype=jnp.int32))
    q1, q2, k1, k2 = [turned(projected[:, i * QK : (i + 1) * QK], cos, sin) for i in range(4)]
    v = projected[:, 4 * QK :].astype(jnp.bfloat16)
    kv = lax.all_gather(jnp.concatenate([k1, k2, v], axis=1), ("z", "y"), axis=0, tiled=True)
    k1, k2, v = kv[:, :QK], kv[:, QK : 2 * QK], kv[:, 2 * QK :]
    lam = lax.dynamic_slice(lambdas, (core,), (1,))
    attended = flash(q1, q2, k1, k2, v, lam, head_gain[None])
    heads = lax.all_gather(attended, "core", axis=1, tiled=True)
    columns = lax.all_gather(out_weight, ("z", "y"), axis=1, tiled=True)
    part = jnp.dot(heads, columns, preferred_element_type=jnp.float32).astype(jnp.bfloat16)
    part = part.reshape(2, 4, 64, 2048)
    got = lax.all_to_all(part, "x", split_axis=1, concat_axis=1, tiled=True)
    summed = got.astype(jnp.float32).sum(axis=1).astype(jnp.bfloat16)
    both_cores = lax.all_to_all(summed[:, :, None], "core", split_axis=0, concat_axis=2, tiled=True)
    out = both_cores.reshape(64, 2, 16, 128)
    return jnp.swapaxes(out, 1, 2).reshape(64, 4096)


def solution(mesh):
    fine = Mesh(mesh.devices.reshape(4, 4, 2, 4), ("z", "y", "core", "x"))
    sp = ("z", "y", "core")
    in_specs = (
        P((*sp, "x"), None),
        P(sp, "x"),
        P(sp, "x"),
        P(sp, "x"),
        P(sp, "x"),
        P(sp, "x"),
        P("x", sp),
        P("x"),
        P(),
    )
    return jax.shard_map(on_device, mesh=fine, in_specs=in_specs, out_specs=P((*sp, "x"), None), check_vma=False)
```

```python
import jax
import jax.numpy as jnp
from jax import lax
from jax.experimental import pallas as pl
from jax.experimental.pallas import tpu as pltpu
from jax.sharding import Mesh, PartitionSpec as P

QK = 128
V = 256
ROPE_BASE = 500000.0
EPS_NORM = 0.02
ROWS = 512
BF = jnp.bfloat16
F32 = jnp.float32
MESH = pl.DeviceIdType.MESH
AXES = ("z", "y", "core", "x")


def rope_tables(positions):
    inverse = 1.0 / ROPE_BASE ** (jnp.arange(0, QK, 2, dtype=F32) / QK)
    angles = positions.astype(F32)[:, None] * inverse[None, :]
    c, s = jnp.cos(angles), jnp.sin(angles)
    return jnp.concatenate([c, c], axis=1), jnp.concatenate([-s, s], axis=1)


def dot(a, b, dims=(((1,), (0,)), ((), ()))):
    return lax.dot_general(a, b, dims, preferred_element_type=F32)


class Links:
    def __init__(self):
        self.at = {a: lax.axis_index(a) for a in AXES}
        self.sent = []

    def peer(self, axis, step):
        n = 2 if axis == "core" else 4
        return {axis: lax.rem(self.at[axis] + (step + n), n)}

    def send(self, src, dst, ssem, rsem, axis, step):
        copy = pltpu.make_async_remote_copy(src, dst, ssem, rsem, device_id=self.peer(axis, step), device_id_type=MESH)
        copy.start()
        self.sent.append(copy)

    def arrived(self, view, ssem, rsem, axis, step):
        pltpu.make_async_remote_copy(view, view, ssem, rsem, device_id=self.peer(axis, step), device_id_type=MESH).wait_recv()

    def drain(self):
        for copy in self.sent:
            copy.wait_send()


NEAR = (0, -1, 1, 2)


class TorusGather:
    def __init__(self, links, piece, ssem, rsem):
        self.links, self.piece, self.ssem, self.rsem = links, piece, ssem, rsem

    def ref(self, half, dp, ds, sub=None):
        dz, dy = (ds, dp) if half == 0 else (dp, ds)
        return self.piece(dz, dy, half, sub)

    def axes(self, half):
        return ("y", "z") if half == 0 else ("z", "y")

    def out(self, half, key, dp, ds, sub, second, step):
        k = half * 20 + key
        view = self.ref(half, dp, ds, sub)
        self.links.send(view, view, self.ssem.at[k], self.rsem.at[k], self.axes(half)[second], step)

    def wait(self, half, key, dp, ds, sub, second, step):
        k = half * 20 + key
        self.links.arrived(self.ref(half, dp, ds, sub), self.ssem.at[k], self.rsem.at[k], self.axes(half)[second], step)

    def spread(self, half, dp):
        i = NEAR.index(dp)
        self.out(half, 4 + 4 * i, dp, 0, None, 1, 1)
        self.out(half, 5 + 4 * i, dp, 0, None, 1, -1)

    def begin(self):
        for half in (0, 1):
            self.out(half, 0, 0, 0, None, 0, 1)
            self.out(half, 1, 0, 0, None, 0, -1)
        for half in (0, 1):
            self.spread(half, 0)

    def first(self):
        for half in (0, 1):
            self.wait(half, 0, -1, 0, None, 0, -1)
            self.out(half, 2, -1, 0, 0, 0, 1)
            self.wait(half, 1, 1, 0, None, 0, 1)
            self.out(half, 3, 1, 0, 1, 0, -1)
        for half in (0, 1):
            self.spread(half, -1)
            self.spread(half, 1)

    def opposite(self):
        for half in (0, 1):
            self.wait(half, 2, 2, 0, 0, 0, -1)
            self.wait(half, 3, 2, 0, 1, 0, 1)
            self.spread(half, 2)

    def second(self, dp, step):
        i = NEAR.index(dp)
        for half in (0, 1):
            if step < 0:
                self.wait(half, 4 + 4 * i, dp, -1, None, 1, -1)
                self.out(half, 6 + 4 * i, dp, -1, 0, 1, 1)
            else:
                self.wait(half, 5 + 4 * i, dp, 1, None, 1, 1)
                self.out(half, 7 + 4 * i, dp, 1, 1, 1, -1)

    def third(self, dp):
        i = NEAR.index(dp)
        for half in (0, 1):
            self.wait(half, 6 + 4 * i, dp, 2, 0, 1, -1)
            self.wait(half, 7 + 4 * i, dp, 2, 1, 1, 1)

    def run(self, chunk, between=()):
        between = dict(between)

        def also(name):
            if name in between:
                between[name]()

        self.first()
        also("first")
        self.second(0, -1)
        chunk(-1, 0)
        chunk(0, -1)
        self.second(0, 1)
        chunk(1, 0)
        chunk(0, 1)
        self.opposite()
        also("opposite")
        self.second(-1, -1)
        chunk(-1, -1)
        self.second(-1, 1)
        also("corner")
        self.second(1, -1)
        chunk(1, -1)
        chunk(-1, 1)
        self.second(1, 1)
        chunk(1, 1)
        self.third(0)
        chunk(0, 2)
        chunk(2, 0)
        self.second(2, -1)
        self.second(2, 1)
        also("far")
        self.third(-1)
        chunk(-1, 2)
        chunk(2, -1)
        self.third(1)
        chunk(1, 2)
        chunk(2, 1)
        self.third(2)
        chunk(2, 2)


def layer_kernel(
    tok, wq1, wq2, wk1, wk2, wv, wo, lam, gain, cos, sin, out,
    tbuf, wbuf, proj, qbuf, kvbuf, obuf, abuf, acc, top, tot,
    fsend, frecv, nsend, nrecv, osend, orecv, mine,
    lsem, wss, wrs, kss, krs, oss, ors, tss, trs, sss, srs, xss, xrs,
):
    links = Links()
    z, y, core, x = [links.at[a] for a in AXES]
    chip = z * 4 + y
    scale = QK ** (-0.5)

    def slot(dz, dy):
        return lax.rem(z + (dz + 4), 4) * 4 + lax.rem(y + (dy + 4), 4)

    barrier = pltpu.get_barrier_semaphore()
    peers = [("core", 1)] + [(a, s) for a in ("x", "y", "z") for s in (1, -1)]
    for axis, step in peers:
        pl.semaphore_signal(barrier, inc=1, device_id=links.peer(axis, step), device_id_type=MESH)
    pl.semaphore_wait(barrier, len(peers))

    own_rows = pl.ds(pl.multiple_of(chip * 256 + core * 128, 128), 128)
    sib_rows = pl.ds(pl.multiple_of(chip * 256 + (1 - core) * 128, 128), 128)
    local = []
    column = 0
    cuts = []
    for i, (w, width) in enumerate(((wq1, QK), (wq2, QK), (wk1, QK), (wk2, QK), (wv, V))):
        here = w.at[:, pl.ds(pl.multiple_of(core * width, 128), width)]
        there = w.at[:, pl.ds(pl.multiple_of((1 - core) * width, 128), width)]
        cols = pl.ds(column, width)
        cuts.append(cols)
        links.send(there, wbuf.at[own_rows, cols], sss.at[i], srs.at[i], "core", 1)
        local.append(pltpu.make_async_copy(here, wbuf.at[own_rows, cols], lsem.at[i]))
        local[-1].start()
        column += width

    def trows(c, dx, sub=None):
        start = c * 256 + lax.rem(x + (dx + 4), 4) * 64
        if sub is None:
            return tbuf.at[pl.ds(pl.multiple_of(start, 64), 64), :]
        return tbuf.at[pl.ds(pl.multiple_of(start + sub * 32, 32), 32), :]

    own_tokens = pltpu.make_async_copy(tok, trows(core, 0), lsem.at[5])
    own_tokens.start()
    links.send(tok, trows(core, 0), tss.at[0], trs.at[0], "x", 1)
    links.send(tok, trows(core, 0), tss.at[1], trs.at[1], "x", -1)
    links.send(tok, trows(core, 0), sss.at[5], srs.at[5], "core", 1)
    own_columns = pl.ds(pl.multiple_of(chip * 128, 128), 128)
    own_out = pltpu.make_async_copy(wo, obuf.at[:, own_columns], lsem.at[6])
    own_out.start()

    for i in range(5):
        local[i].wait()
        links.arrived(wbuf.at[sib_rows, cuts[i]], sss.at[i], srs.at[i], "core", 1)

    def wpiece(dz, dy, half, sub):
        start = slot(dz, dy) * 256 + half * 128
        if sub is None:
            return wbuf.at[pl.ds(pl.multiple_of(start, 128), 128), :]
        return wbuf.at[pl.ds(pl.multiple_of(start + sub * 64, 64), 64), :]

    weights = TorusGather(links, wpiece, wss, wrs)
    weights.begin()

    pending = []
    ready = []

    def project(dz, dy):
        if not ready:
            pending.append((dz, dy))
            return
        depth = pl.ds(pl.multiple_of(slot(dz, dy) * 256, 256), 256)
        term = dot(tbuf[:, depth], wbuf[depth, :])
        if len(ready) == 1:
            proj[...] = term
            ready.append(1)
        else:
            proj[...] += term

    def near_tokens():
        links.arrived(trows(core, -1), tss.at[0], trs.at[0], "x", -1)
        links.send(trows(core, -1, 0), trows(core, -1, 0), tss.at[2], trs.at[2], "x", 1)
        links.send(trows(core, -1), trows(core, -1), sss.at[6], srs.at[6], "core", 1)
        links.arrived(trows(core, 1), tss.at[1], trs.at[1], "x", 1)
        links.send(trows(core, 1, 1), trows(core, 1, 1), tss.at[3], trs.at[3], "x", -1)
        links.send(trows(core, 1), trows(core, 1), sss.at[7], srs.at[7], "core", 1)

    def far_tokens():
        links.arrived(trows(core, 2, 0), tss.at[2], trs.at[2], "x", -1)
        links.arrived(trows(core, 2, 1), tss.at[3], trs.at[3], "x", 1)
        links.send(trows(core, 2), trows(core, 2), sss.at[8], srs.at[8], "core", 1)
        own_tokens.wait()
        for i, dx in ((5, 0), (6, -1), (7, 1), (8, 2)):
            links.arrived(trows(1 - core, dx), sss.at[i], srs.at[i], "core", 1)
        ready.append(1)
        for item in [(0, 0)] + pending:
            project(*item)

    weights.run(project, {"opposite": near_tokens, "corner": far_tokens})

    def opiece(dz, dy, half, sub):
        cols = pl.ds(pl.multiple_of(slot(dz, dy) * 128, 128), 128)
        if sub is None:
            return obuf.at[pl.ds(half * 256, 256), cols]
        return obuf.at[pl.ds(half * 256 + sub * 128, 128), cols]

    own_out.wait()
    columns = TorusGather(links, opiece, oss, ors)
    columns.begin()

    def turned(i):
        v = proj[:, i * QK : (i + 1) * QK]
        swapped = jnp.concatenate([v[:, QK // 2 :], v[:, : QK // 2]], axis=1)
        return (v * cos[...] + swapped * sin[...]).astype(BF)

    own_keys = pl.ds(pl.multiple_of(chip * ROWS, ROWS), ROWS)
    kvbuf[own_keys, 0:QK] = turned(2)
    kvbuf[own_keys, QK : 2 * QK] = turned(3)
    kvbuf[own_keys, 2 * QK :] = proj[:, 4 * QK :].astype(BF)

    def kpiece(dz, dy, half, sub):
        start = slot(dz, dy) * ROWS + half * 256
        if sub is None:
            return kvbuf.at[pl.ds(pl.multiple_of(start, 256), 256), :]
        return kvbuf.at[pl.ds(pl.multiple_of(start + sub * 128, 128), 128), :]

    keys = TorusGather(links, kpiece, kss, krs)
    keys.begin()
    qbuf[0] = turned(0)
    qbuf[1] = turned(1)

    def attend(index, diagonal):
        start = pl.multiple_of(index * ROWS, ROWS)
        span = pl.ds(start, ROWS)
        v = kvbuf[span, 2 * QK :]
        for a in range(2):
            s = dot(qbuf[a], kvbuf[span, a * QK : (a + 1) * QK], (((1,), (1,)), ((), ()))) * scale
            if diagonal:
                rows = lax.broadcasted_iota(jnp.int32, s.shape, 0)
                cols = lax.broadcasted_iota(jnp.int32, s.shape, 1)
                s = jnp.where(cols <= rows, s, -1e30)
                new = jnp.max(s, axis=1, keepdims=True)
                e = jnp.exp(s - new)
                tot[a] = jnp.broadcast_to(jnp.sum(e, axis=1, keepdims=True), (ROWS, 128))
                acc[a] = dot(e.astype(BF), v)
            else:
                old = top[a][:, :1]
                new = jnp.maximum(old, jnp.max(s, axis=1, keepdims=True))
                e = jnp.exp(s - new)
                fade = jnp.exp(old - new)
                tot[a] = tot[a] * fade + jnp.sum(e, axis=1, keepdims=True)
                acc[a] = acc[a] * fade + dot(e.astype(BF), v)
            top[a] = jnp.broadcast_to(new, (ROWS, 128))

    attend(chip, True)

    def chunk(dz, dy):
        index = slot(dz, dy)

        @pl.when(index < chip)
        def _():
            attend(index, False)

    columns.first()
    for dp in (0,):
        columns.second(dp, -1)
        columns.second(dp, 1)
    columns.opposite()
    for dp in (-1, 1, 2):
        columns.second(dp, -1)
        columns.second(dp, 1)
    for dp in NEAR:
        columns.third(dp)
    keys.run(chunk)

    o1 = acc[0] / tot[0][:, :1]
    o2 = acc[1] / tot[1][:, :1]
    mixed = o1 - lam[core] * o2
    norm = lax.rsqrt(jnp.mean(mixed * mixed, axis=1, keepdims=True) + EPS_NORM)
    mine[...] = (mixed * norm * gain[...]).astype(BF)
    links.send(mine, abuf.at[core], xss.at[0], xrs.at[0], "core", 1)
    keep = pltpu.make_async_copy(mine, abuf.at[core], lsem.at[7])
    keep.start()
    keep.wait()
    links.arrived(abuf.at[1 - core], xss.at[0], xrs.at[0], "core", 1)

    def partial(dx, r):
        start = r * 256 + lax.rem(x + (dx + 4), 4) * 64
        rows = pl.ds(pl.multiple_of(start, 64), 64)
        return dot(abuf[0, rows, :], obuf[0:256, :]) + dot(abuf[1, rows, :], obuf[256:512, :])

    for r in (0, 1):
        fsend[r] = partial(2, r).astype(BF)
        step = 1 if r == 0 else -1
        links.send(fsend.at[r], frecv.at[r], xss.at[1 + r], xrs.at[1 + r], "x", step)
    for r in (0, 1):
        step = -1 if r == 0 else 1
        nsend[r, r] = partial(step, r).astype(BF)
        links.send(nsend.at[r, r], nrecv.at[r, r], xss.at[3 + r], xrs.at[3 + r], "x", step)
    for r in (0, 1):
        step = 1 if r == 0 else -1
        term = partial(step, r)
        links.arrived(frecv.at[r], xss.at[1 + r], xrs.at[1 + r], "x", -step)
        nsend[1 - r, r] = (term + frecv[r].astype(F32)).astype(BF)
        links.send(nsend.at[1 - r, r], nrecv.at[1 - r, r], xss.at[5 + r], xrs.at[5 + r], "x", step)
    sums = [partial(0, 0), partial(0, 1)]
    for r in (0, 1):
        step = -1 if r == 0 else 1
        links.arrived(nrecv.at[r, r], xss.at[3 + r], xrs.at[3 + r], "x", -step)
        sums[r] = sums[r] + nrecv[r, r].astype(F32)
    for r in (0, 1):
        step = 1 if r == 0 else -1
        links.arrived(nrecv.at[1 - r, r], xss.at[5 + r], xrs.at[5 + r], "x", -step)
        osend[r] = (sums[r] + nrecv[1 - r, r].astype(F32)).astype(BF)
    links.send(osend.at[1 - core], orecv, xss.at[7], xrs.at[7], "core", 1)
    links.arrived(orecv, xss.at[7], xrs.at[7], "core", 1)
    own = osend[core]
    other = orecv[...]
    low = jnp.where(core == 0, own, other)
    high = jnp.where(core == 0, other, own)
    for k in range(16):
        out[:, k * 256 : k * 256 + 128] = low[:, k * 128 : (k + 1) * 128]
        out[:, k * 256 + 128 : k * 256 + 256] = high[:, k * 128 : (k + 1) * 128]
    links.drain()


def on_device(tokens, query_one, query_two, key_one, key_two, value_weight, out_weight, lambdas, head_gain):
    chip = lax.axis_index("z") * 4 + lax.axis_index("y")
    cos, sin = rope_tables(chip * ROWS + jnp.arange(ROWS, dtype=jnp.int32))
    vm = pl.BlockSpec(memory_space=pltpu.VMEM)
    dma = pltpu.SemaphoreType.DMA
    return pl.pallas_call(
        layer_kernel,
        out_shape=jax.ShapeDtypeStruct((64, 4096), BF),
        in_specs=[vm] * 7 + [pl.BlockSpec(memory_space=pltpu.SMEM)] + [vm] * 3,
        out_specs=vm,
        scratch_shapes=[
            pltpu.VMEM((512, 4096), BF),
            pltpu.VMEM((4096, 768), BF),
            pltpu.VMEM((ROWS, 768), F32),
            pltpu.VMEM((2, ROWS, QK), BF),
            pltpu.VMEM((8192, 512), BF),
            pltpu.VMEM((512, 2048), BF),
            pltpu.VMEM((2, ROWS, V), BF),
            pltpu.VMEM((2, ROWS, V), F32),
            pltpu.VMEM((2, ROWS, 128), F32),
            pltpu.VMEM((2, ROWS, 128), F32),
            pltpu.VMEM((2, 64, 2048), BF),
            pltpu.VMEM((2, 64, 2048), BF),
            pltpu.VMEM((2, 2, 64, 2048), BF),
            pltpu.VMEM((2, 2, 64, 2048), BF),
            pltpu.VMEM((2, 64, 2048), BF),
            pltpu.VMEM((64, 2048), BF),
            pltpu.VMEM((ROWS, V), BF),
            dma((8,)),
            dma((40,)), dma((40,)),
            dma((40,)), dma((40,)),
            dma((40,)), dma((40,)),
            dma((4,)), dma((4,)),
            dma((9,)), dma((9,)),
            dma((8,)), dma((8,)),
        ],
        compiler_params=pltpu.CompilerParams(
            collective_id=0, has_side_effects=True, vmem_limit_bytes=60 * 1024 * 1024
        ),
    )(tokens, query_one, query_two, key_one, key_two, value_weight, out_weight, lambdas, head_gain[None], cos, sin)


def solution(mesh):
    fine = Mesh(mesh.devices.reshape(4, 4, 2, 4), AXES)
    sp = ("z", "y", "core")
    in_specs = (
        P((*sp, "x"), None),
        P(sp, "x"),
        P(sp, "x"),
        P(sp, "x"),
        P(sp, "x"),
        P(sp, "x"),
        P("x", sp),
        P("x"),
        P(),
    )
    return jax.shard_map(on_device, mesh=fine, in_specs=in_specs, out_specs=P((*sp, "x"), None), check_vma=False)
```

```python
import jax
import jax.numpy as jnp
import numpy as np
from jax import lax
from jax.experimental import pallas as pl
from jax.experimental.pallas import tpu as pltpu
from jax.sharding import Mesh, PartitionSpec as P

QK = 128
V = 256
ROPE_BASE = 500000.0
EPS_NORM = 0.02
LOG2E = 1.4426950408889634
ROWS = 512
BF = jnp.bfloat16
F32 = jnp.float32
MESH = pl.DeviceIdType.MESH
AXES = ("z", "y", "core", "x")


def dot(a, b, dims=(((1,), (0,)), ((), ()))):
    return lax.dot_general(a, b, dims, preferred_element_type=F32)


class Links:
    def __init__(self):
        self.at = {a: lax.axis_index(a) for a in AXES}
        self.sent = []

    def peer(self, axis, step):
        n = 2 if axis == "core" else 4
        return {axis: lax.rem(self.at[axis] + (step + n), n)}

    def send(self, views, axis, step):
        def copy():
            return pltpu.make_async_remote_copy(*views(), device_id=self.peer(axis, step), device_id_type=MESH)

        copy().start()
        self.sent.append(copy)

    def arrived(self, view, ssem, rsem, axis, step):
        pltpu.make_async_remote_copy(view, view, ssem, rsem, device_id=self.peer(axis, step), device_id_type=MESH).wait_recv()

    def drain(self):
        for copy in self.sent:
            copy().wait_send()


NEAR = (0, -1, 1, 2)


class TorusGather:
    def __init__(self, links, piece, ssem, rsem):
        self.links, self.piece, self.ssem, self.rsem = links, piece, ssem, rsem

    def ref(self, half, dp, ds, sub=None):
        dz, dy = (ds, dp) if half == 0 else (dp, ds)
        return self.piece(dz, dy, half, sub)

    def axes(self, half):
        return ("y", "z") if half == 0 else ("z", "y")

    def out(self, half, key, dp, ds, sub, second, step):
        k = half * 20 + key
        def views():
            view = self.ref(half, dp, ds, sub)
            return view, view, self.ssem.at[k], self.rsem.at[k]

        self.links.send(views, self.axes(half)[second], step)

    def wait(self, half, key, dp, ds, sub, second, step):
        k = half * 20 + key
        self.links.arrived(self.ref(half, dp, ds, sub), self.ssem.at[k], self.rsem.at[k], self.axes(half)[second], step)

    def spread(self, half, dp):
        i = NEAR.index(dp)
        self.out(half, 4 + 4 * i, dp, 0, None, 1, 1)
        self.out(half, 5 + 4 * i, dp, 0, None, 1, -1)

    def begin(self):
        for half in (0, 1):
            self.out(half, 0, 0, 0, None, 0, 1)
            self.out(half, 1, 0, 0, None, 0, -1)
        for half in (0, 1):
            self.spread(half, 0)

    def first(self):
        for half in (0, 1):
            self.wait(half, 0, -1, 0, None, 0, -1)
            self.out(half, 2, -1, 0, 0, 0, 1)
            self.wait(half, 1, 1, 0, None, 0, 1)
            self.out(half, 3, 1, 0, 1, 0, -1)
        for half in (0, 1):
            self.spread(half, -1)
            self.spread(half, 1)

    def opposite(self):
        for half in (0, 1):
            self.wait(half, 2, 2, 0, 0, 0, -1)
            self.wait(half, 3, 2, 0, 1, 0, 1)
            self.spread(half, 2)

    def second(self, dp, step):
        i = NEAR.index(dp)
        for half in (0, 1):
            if step < 0:
                self.wait(half, 4 + 4 * i, dp, -1, None, 1, -1)
                self.out(half, 6 + 4 * i, dp, -1, 0, 1, 1)
            else:
                self.wait(half, 5 + 4 * i, dp, 1, None, 1, 1)
                self.out(half, 7 + 4 * i, dp, 1, 1, 1, -1)

    def third(self, dp):
        i = NEAR.index(dp)
        for half in (0, 1):
            self.wait(half, 6 + 4 * i, dp, 2, 0, 1, -1)
            self.wait(half, 7 + 4 * i, dp, 2, 1, 1, 1)

    def steps(self):
        second, third = self.second, self.third
        return [
            ([self.first, lambda: second(0, -1)], (-1, 0)),
            ([], (0, -1)),
            ([lambda: second(0, 1)], (1, 0)),
            ([], (0, 1)),
            ([self.opposite, lambda: second(-1, -1)], (-1, -1)),
            ([lambda: second(-1, 1), lambda: second(1, -1)], (1, -1)),
            ([], (-1, 1)),
            ([lambda: second(1, 1)], (1, 1)),
            ([lambda: third(0)], (0, 2)),
            ([], (2, 0)),
            ([lambda: second(2, -1), lambda: second(2, 1), lambda: third(-1)], (-1, 2)),
            ([], (2, -1)),
            ([lambda: third(1)], (1, 2)),
            ([], (2, 1)),
            ([lambda: third(2)], (2, 2)),
        ]


def pick(t, values):
    result = values[0]
    for k in range(1, len(values)):
        result = jnp.where(t == k, values[k], result)
    return result


def on_step(t, k, actions):
    if actions:

        @pl.when(t == k)
        def _():
            for action in actions:
                action()


def layer_kernel(
    tok, wq1, wq2, wk1, wk2, wv, wo, lam, gain, inverse, out, cos, sin,
    tbuf, wbuf, proj, qbuf, kvbuf, obuf, abuf, acc, top, tot,
    fsend, frecv, nsend, nrecv, osend, orecv, mine,
    lsem, wss, wrs, kss, krs, oss, ors, tss, trs, sss, srs, xss, xrs,
):
    links = Links()
    z, y, core, x = [links.at[a] for a in AXES]
    chip = z * 4 + y
    scale = QK ** (-0.5)

    def slot(dz, dy):
        return lax.rem(z + (dz + 4), 4) * 4 + lax.rem(y + (dy + 4), 4)

    def plain(src, dst, ssem, rsem, axis, step):
        links.send(lambda: (src, dst, ssem, rsem), axis, step)

    barrier = pltpu.get_barrier_semaphore()
    peers = [("core", 1)] + [(a, s) for a in ("x", "y", "z") for s in (1, -1)]
    for axis, step in peers:
        pl.semaphore_signal(barrier, inc=1, device_id=links.peer(axis, step), device_id_type=MESH)
    pl.semaphore_wait(barrier, len(peers))

    own_rows = pl.ds(pl.multiple_of(chip * 256 + core * 128, 128), 128)
    sib_rows = pl.ds(pl.multiple_of(chip * 256 + (1 - core) * 128, 128), 128)
    local = []
    column = 0
    cuts = []
    for i, (w, width) in enumerate(((wq1, QK), (wq2, QK), (wk1, QK), (wk2, QK), (wv, V))):
        here = w.at[:, pl.ds(pl.multiple_of(core * width, 128), width)]
        there = w.at[:, pl.ds(pl.multiple_of((1 - core) * width, 128), width)]
        cols = pl.ds(column, width)
        cuts.append(cols)
        plain(there, wbuf.at[own_rows, cols], sss.at[i], srs.at[i], "core", 1)
        local.append(pltpu.make_async_copy(here, wbuf.at[own_rows, cols], lsem.at[i]))
        local[-1].start()
        column += width

    def trows(c, dx, sub=None):
        start = c * 256 + lax.rem(x + (dx + 4), 4) * 64
        if sub is None:
            return tbuf.at[pl.ds(pl.multiple_of(start, 64), 64), :]
        return tbuf.at[pl.ds(pl.multiple_of(start + sub * 32, 32), 32), :]

    own_tokens = pltpu.make_async_copy(tok, trows(core, 0), lsem.at[5])
    own_tokens.start()
    plain(tok, trows(core, 0), tss.at[0], trs.at[0], "x", 1)
    plain(tok, trows(core, 0), tss.at[1], trs.at[1], "x", -1)
    plain(tok, trows(core, 0), sss.at[5], srs.at[5], "core", 1)
    own_columns = pl.ds(pl.multiple_of(chip * 128, 128), 128)
    own_out = pltpu.make_async_copy(wo, obuf.at[:, own_columns], lsem.at[6])
    own_out.start()

    for i in range(5):
        local[i].wait()
        links.arrived(wbuf.at[sib_rows, cuts[i]], sss.at[i], srs.at[i], "core", 1)

    def wpiece(dz, dy, half, sub):
        start = slot(dz, dy) * 256 + half * 128
        if sub is None:
            return wbuf.at[pl.ds(pl.multiple_of(start, 128), 128), :]
        return wbuf.at[pl.ds(pl.multiple_of(start + sub * 64, 64), 64), :]

    weights = TorusGather(links, wpiece, wss, wrs)
    weights.begin()

    def pass_on(dx, sub, ssem, rsem, i, axis, step):
        def views():
            return trows(core, dx, sub), trows(core, dx, sub), ssem.at[i], rsem.at[i]

        links.send(views, axis, step)

    def near_tokens():
        links.arrived(trows(core, -1), tss.at[0], trs.at[0], "x", -1)
        pass_on(-1, 0, tss, trs, 2, "x", 1)
        pass_on(-1, None, sss, srs, 6, "core", 1)
        links.arrived(trows(core, 1), tss.at[1], trs.at[1], "x", 1)
        pass_on(1, 1, tss, trs, 3, "x", -1)
        pass_on(1, None, sss, srs, 7, "core", 1)

    def far_tokens():
        links.arrived(trows(core, 2, 0), tss.at[2], trs.at[2], "x", -1)
        links.arrived(trows(core, 2, 1), tss.at[3], trs.at[3], "x", 1)
        pass_on(2, None, sss, srs, 8, "core", 1)
        own_tokens.wait()
        for i, dx in ((5, 0), (6, -1), (7, 1), (8, 2)):
            links.arrived(trows(1 - core, dx), sss.at[i], srs.at[i], "core", 1)

    steps = weights.steps()
    early = [action for actions, _ in steps[:5] for action in actions] + [near_tokens]
    early += [action for actions, _ in steps[5:8] for action in actions] + [far_tokens]
    dzs = [0] + [d for _, (d, _) in steps]
    dys = [0] + [d for _, (_, d) in steps]
    proj[...] = jnp.zeros_like(proj)
    half_dim = QK // 2
    position = chip * ROWS + lax.broadcasted_iota(jnp.int32, (ROWS, half_dim), 0)
    angle = position.astype(F32) * inverse[...]
    cos_part, sin_part = jnp.cos(angle), jnp.sin(angle)
    cos[:, :half_dim] = cos_part
    cos[:, half_dim:] = cos_part
    sin[:, :half_dim] = -sin_part
    sin[:, half_dim:] = sin_part

    @pl.loop(0, 16)
    def _(t):
        on_step(t, 0, early)
        for k in range(9, 16):
            on_step(t, k, steps[k - 1][0])
        depth = pl.ds(pl.multiple_of(slot(pick(t, dzs), pick(t, dys)) * 256, 256), 256)
        proj[...] += dot(tbuf[:, depth], wbuf[depth, :])


    def opiece(dz, dy, half, sub):
        cols = pl.ds(pl.multiple_of(slot(dz, dy) * 128, 128), 128)
        if sub is None:
            return obuf.at[pl.ds(half * 256, 256), cols]
        return obuf.at[pl.ds(half * 256 + sub * 128, 128), cols]

    own_out.wait()
    columns = TorusGather(links, opiece, oss, ors)
    columns.begin()

    def turned(i):
        v = proj[:, i * QK : (i + 1) * QK]
        swapped = jnp.concatenate([v[:, QK // 2 :], v[:, : QK // 2]], axis=1)
        return (v * cos[...] + swapped * sin[...]).astype(BF)

    own_keys = pl.ds(pl.multiple_of(chip * ROWS, ROWS), ROWS)
    kvbuf[own_keys, 0:QK] = turned(2)
    kvbuf[own_keys, QK : 2 * QK] = turned(3)
    kvbuf[own_keys, 2 * QK :] = proj[:, 4 * QK :].astype(BF)

    def kpiece(dz, dy, half, sub):
        start = slot(dz, dy) * ROWS + half * 256
        if sub is None:
            return kvbuf.at[pl.ds(pl.multiple_of(start, 256), 256), :]
        return kvbuf.at[pl.ds(pl.multiple_of(start + sub * 128, 128), 128), :]

    keys = TorusGather(links, kpiece, kss, krs)
    keys.begin()
    qbuf[0] = turned(0)
    qbuf[1] = turned(1)

    log_scale = scale * LOG2E

    def attend(index, diagonal):
        span = pl.ds(pl.multiple_of(index * ROWS, ROWS), ROWS)
        v = kvbuf[span, 2 * QK :]
        for r in range(2):
            rows = pl.ds(r * 256, 256)
            for a in range(2):
                s = dot(qbuf[a, rows], kvbuf[span, a * QK : (a + 1) * QK], (((1,), (1,)), ((), ())))
                if diagonal:
                    row_ids = r * 256 + lax.broadcasted_iota(jnp.int32, s.shape, 0)
                    s = jnp.where(lax.broadcasted_iota(jnp.int32, s.shape, 1) <= row_ids, s, -1e30)
                parts = [s[:, k * 128 : (k + 1) * 128] for k in range(4)]
                high = jnp.maximum(jnp.maximum(parts[0], parts[1]), jnp.maximum(parts[2], parts[3]))
                high = jnp.max(high, axis=1, keepdims=True) * log_scale
                if diagonal:
                    new = high
                else:
                    old = top[a, rows][:, :1]
                    new = jnp.maximum(old, high)
                e = jnp.exp2(s * log_scale - new)
                total = (e[:, 0:128] + e[:, 128:256]) + (e[:, 256:384] + e[:, 384:512])
                weighted = dot(e.astype(BF), v)
                if diagonal:
                    tot[a, rows] = total
                    acc[a, rows] = weighted
                else:
                    fade = jnp.exp2(old - new)
                    tot[a, rows] = tot[a, rows] * fade + total
                    acc[a, rows] = acc[a, rows] * fade + weighted
                top[a, rows] = jnp.broadcast_to(new, (256, 128))

    attend(chip, True)

    columns.first()
    for dp in (0,):
        columns.second(dp, -1)
        columns.second(dp, 1)
    columns.opposite()
    for dp in (-1, 1, 2):
        columns.second(dp, -1)
        columns.second(dp, 1)
    for dp in NEAR:
        columns.third(dp)
    ksteps = keys.steps()

    @pl.loop(0, 15)
    def _(t):
        for k in range(15):
            on_step(t, k, ksteps[k][0])
        index = slot(pick(t, dzs[1:]), pick(t, dys[1:]))

        @pl.when(index < chip)
        def _():
            attend(index, False)

    o1 = acc[0] / jnp.sum(tot[0], axis=1, keepdims=True)
    o2 = acc[1] / jnp.sum(tot[1], axis=1, keepdims=True)
    mixed = o1 - lam[core] * o2
    norm = lax.rsqrt(jnp.mean(mixed * mixed, axis=1, keepdims=True) + EPS_NORM)
    mine[...] = (mixed * norm * gain[...]).astype(BF)
    plain(mine, abuf.at[core], xss.at[0], xrs.at[0], "core", 1)
    keep = pltpu.make_async_copy(mine, abuf.at[core], lsem.at[7])
    keep.start()
    keep.wait()
    links.arrived(abuf.at[1 - core], xss.at[0], xrs.at[0], "core", 1)

    def partial(dx, r):
        start = r * 256 + lax.rem(x + (dx + 4), 4) * 64
        rows = pl.ds(pl.multiple_of(start, 64), 64)
        return dot(abuf[0, rows, :], obuf[0:256, :]) + dot(abuf[1, rows, :], obuf[256:512, :])

    for r in (0, 1):
        fsend[r] = partial(2, r).astype(BF)
        step = 1 if r == 0 else -1
        plain(fsend.at[r], frecv.at[r], xss.at[1 + r], xrs.at[1 + r], "x", step)
    for r in (0, 1):
        step = -1 if r == 0 else 1
        nsend[r, r] = partial(step, r).astype(BF)
        plain(nsend.at[r, r], nrecv.at[r, r], xss.at[3 + r], xrs.at[3 + r], "x", step)
    for r in (0, 1):
        step = 1 if r == 0 else -1
        term = partial(step, r)
        links.arrived(frecv.at[r], xss.at[1 + r], xrs.at[1 + r], "x", -step)
        nsend[1 - r, r] = (term + frecv[r].astype(F32)).astype(BF)
        plain(nsend.at[1 - r, r], nrecv.at[1 - r, r], xss.at[5 + r], xrs.at[5 + r], "x", step)
    sums = [partial(0, 0), partial(0, 1)]
    for r in (0, 1):
        step = -1 if r == 0 else 1
        links.arrived(nrecv.at[r, r], xss.at[3 + r], xrs.at[3 + r], "x", -step)
        sums[r] = sums[r] + nrecv[r, r].astype(F32)
    for r in (0, 1):
        step = 1 if r == 0 else -1
        links.arrived(nrecv.at[1 - r, r], xss.at[5 + r], xrs.at[5 + r], "x", -step)
        osend[r] = (sums[r] + nrecv[1 - r, r].astype(F32)).astype(BF)
    plain(osend.at[1 - core], orecv, xss.at[7], xrs.at[7], "core", 1)
    links.arrived(orecv, xss.at[7], xrs.at[7], "core", 1)
    own = osend[core]
    other = orecv[...]
    low = jnp.where(core == 0, own, other)
    high = jnp.where(core == 0, other, own)
    for k in range(16):
        out[:, k * 256 : k * 256 + 128] = low[:, k * 128 : (k + 1) * 128]
        out[:, k * 256 + 128 : k * 256 + 256] = high[:, k * 128 : (k + 1) * 128]
    links.drain()


def on_device(tokens, query_one, query_two, key_one, key_two, value_weight, out_weight, lambdas, head_gain):
    inverse = 1.0 / np.float32(ROPE_BASE) ** (np.arange(0, QK, 2, dtype=np.float32) / np.float32(QK))
    vm = pl.BlockSpec(memory_space=pltpu.VMEM)
    dma = pltpu.SemaphoreType.DMA
    return pl.pallas_call(
        layer_kernel,
        out_shape=jax.ShapeDtypeStruct((64, 4096), BF),
        in_specs=[vm] * 7 + [pl.BlockSpec(memory_space=pltpu.SMEM)] + [vm] * 2,
        out_specs=vm,
        scratch_shapes=[
            pltpu.VMEM((ROWS, QK), F32),
            pltpu.VMEM((ROWS, QK), F32),
            pltpu.VMEM((512, 4096), BF),
            pltpu.VMEM((4096, 768), BF),
            pltpu.VMEM((ROWS, 768), F32),
            pltpu.VMEM((2, ROWS, QK), BF),
            pltpu.VMEM((8192, 512), BF),
            pltpu.VMEM((512, 2048), BF),
            pltpu.VMEM((2, ROWS, V), BF),
            pltpu.VMEM((2, ROWS, V), F32),
            pltpu.VMEM((2, ROWS, 128), F32),
            pltpu.VMEM((2, ROWS, 128), F32),
            pltpu.VMEM((2, 64, 2048), BF),
            pltpu.VMEM((2, 64, 2048), BF),
            pltpu.VMEM((2, 2, 64, 2048), BF),
            pltpu.VMEM((2, 2, 64, 2048), BF),
            pltpu.VMEM((2, 64, 2048), BF),
            pltpu.VMEM((64, 2048), BF),
            pltpu.VMEM((ROWS, V), BF),
            dma((8,)),
            dma((40,)), dma((40,)),
            dma((40,)), dma((40,)),
            dma((40,)), dma((40,)),
            dma((4,)), dma((4,)),
            dma((9,)), dma((9,)),
            dma((8,)), dma((8,)),
        ],
        compiler_params=pltpu.CompilerParams(
            collective_id=0, has_side_effects=True, vmem_limit_bytes=60 * 1024 * 1024
        ),
    )(tokens, query_one, query_two, key_one, key_two, value_weight, out_weight, lambdas, head_gain[None], jnp.asarray(inverse[None], F32))


def solution(mesh):
    fine = Mesh(mesh.devices.reshape(4, 4, 2, 4), AXES)
    sp = ("z", "y", "core")
    in_specs = (
        P((*sp, "x"), None),
        P(sp, "x"),
        P(sp, "x"),
        P(sp, "x"),
        P(sp, "x"),
        P(sp, "x"),
        P("x", sp),
        P("x"),
        P(),
    )
    return jax.shard_map(on_device, mesh=fine, in_specs=in_specs, out_specs=P((*sp, "x"), None), check_vma=False)
```

```python
import jax
import jax.numpy as jnp
import numpy as np
from jax import lax
from jax.experimental import pallas as pl
from jax.experimental.pallas import tpu as pltpu
from jax.sharding import Mesh, PartitionSpec as P

QK = 128
V = 256
ROPE_BASE = 500000.0
EPS_NORM = 0.02
LOG2E = 1.4426950408889634
ROWS = 512
BF = jnp.bfloat16
F32 = jnp.float32
MESH = pl.DeviceIdType.MESH
AXES = ("z", "y", "core", "x")
NEAR = (0, -1, 1, 2)


def dot(a, b, dims=(((1,), (0,)), ((), ()))):
    return lax.dot_general(a, b, dims, preferred_element_type=F32)


class Links:
    def __init__(self):
        self.z, self.y, self.core, self.x = [lax.axis_index(a) for a in AXES]
        self.u = self.y * (1 - self.core) + self.x * self.core
        self.w = self.x * (1 - self.core) + self.y * self.core
        self.sent = []

    def peer(self, axis, step):
        if axis == "core":
            return {"core": 1 - self.core}
        if axis == "even":
            return {"core": 0}
        if axis == "odd":
            return {"y": self.x, "core": 1, "x": self.y}
        if axis == "z":
            return {"z": lax.rem(self.z + (step + 4), 4)}
        along = self.core if axis == "u" else 1 - self.core
        return {"y": lax.rem(self.y + (4 + step * (1 - along)), 4), "x": lax.rem(self.x + (4 + step * along), 4)}

    def send(self, views, axis, step, only=None):
        def copy():
            return pltpu.make_async_remote_copy(*views(), device_id=self.peer(axis, step), device_id_type=MESH)

        if only is None:
            copy().start()
        else:
            pl.when(only)(lambda: copy().start())
        self.sent.append((copy, only))

    def arrived(self, view, ssem, rsem):
        pltpu.make_async_remote_copy(view, view, ssem, rsem, device_id=self.peer("core", 1), device_id_type=MESH).wait_recv()

    def drain(self):
        for copy, only in self.sent:
            if only is None:
                copy().wait_send()
            else:
                pl.when(only)(lambda copy=copy: copy().wait_send())


class TorusGather:
    def __init__(self, links, piece, ssem, rsem):
        self.links, self.piece, self.ssem, self.rsem = links, piece, ssem, rsem

    def ref(self, part, dp, ds, sub=None):
        dz, du = (ds, dp) if part == 0 else (dp, ds)
        return self.piece(dz, du, part, sub)

    def axis(self, part, second):
        return ("u", "z")[part ^ second]

    def out(self, part, key, dp, ds, sub, second, step):
        k = part * 20 + key

        def views():
            view = self.ref(part, dp, ds, sub)
            return view, view, self.ssem.at[k], self.rsem.at[k]

        self.links.send(views, self.axis(part, second), step)

    def wait(self, part, key, dp, ds, sub):
        k = part * 20 + key
        self.links.arrived(self.ref(part, dp, ds, sub), self.ssem.at[k], self.rsem.at[k])

    def spread(self, part, dp):
        i = NEAR.index(dp)
        self.out(part, 4 + 4 * i, dp, 0, None, 1, 1)
        self.out(part, 5 + 4 * i, dp, 0, None, 1, -1)

    def begin(self):
        for part in (0, 1):
            self.out(part, 0, 0, 0, None, 0, 1)
            self.out(part, 1, 0, 0, None, 0, -1)
        for part in (0, 1):
            self.spread(part, 0)

    def first(self):
        for part in (0, 1):
            self.wait(part, 0, -1, 0, None)
            self.out(part, 2, -1, 0, 0, 0, 1)
            self.wait(part, 1, 1, 0, None)
            self.out(part, 3, 1, 0, 1, 0, -1)
        for part in (0, 1):
            self.spread(part, -1)
            self.spread(part, 1)

    def opposite(self):
        for part in (0, 1):
            self.wait(part, 2, 2, 0, 0)
            self.wait(part, 3, 2, 0, 1)
            self.spread(part, 2)

    def second(self, dp, step):
        i = NEAR.index(dp)
        for part in (0, 1):
            if step < 0:
                self.wait(part, 4 + 4 * i, dp, -1, None)
                self.out(part, 6 + 4 * i, dp, -1, 0, 1, 1)
            else:
                self.wait(part, 5 + 4 * i, dp, 1, None)
                self.out(part, 7 + 4 * i, dp, 1, 1, 1, -1)

    def third(self, dp):
        i = NEAR.index(dp)
        for part in (0, 1):
            self.wait(part, 6 + 4 * i, dp, 2, 0)
            self.wait(part, 7 + 4 * i, dp, 2, 1)

    def steps(self):
        second, third = self.second, self.third
        return [
            ([self.first, lambda: second(0, -1)], (-1, 0)),
            ([], (0, -1)),
            ([lambda: second(0, 1)], (1, 0)),
            ([], (0, 1)),
            ([self.opposite, lambda: second(-1, -1)], (-1, -1)),
            ([lambda: second(-1, 1), lambda: second(1, -1)], (1, -1)),
            ([], (-1, 1)),
            ([lambda: second(1, 1)], (1, 1)),
            ([lambda: third(0)], (0, 2)),
            ([], (2, 0)),
            ([lambda: second(2, -1), lambda: second(2, 1), lambda: third(-1)], (-1, 2)),
            ([], (2, -1)),
            ([lambda: third(1)], (1, 2)),
            ([], (2, 1)),
            ([lambda: third(2)], (2, 2)),
        ]


def pick(t, values):
    result = values[0]
    for k in range(1, len(values)):
        result = jnp.where(t == k, values[k], result)
    return result


def on_step(t, k, actions):
    if actions:

        @pl.when(t == k)
        def _():
            for action in actions:
                action()


def window(start, size):
    return pl.ds(pl.multiple_of(start, size), size)


def layer_kernel(
    tok, wq1, wq2, wk1, wk2, wv, wo, lam, gain, inverse, out, cos, sin,
    tbuf, wbuf, proj, qbuf, kvbuf, obuf, acc, top, tot,
    fsend, frecv, nsend, nrecv, keep, sums, osend, orecv, mine, lown, lrecv,
    lsem, wss, wrs, kss, krs, oss, ors, tss, trs, sss, srs, xss, xrs,
):
    links = Links()
    z, y, core, x, u, w = links.z, links.y, links.core, links.x, links.u, links.w
    chip = z * 4 + y
    place = z * 4 + u
    log_scale = QK ** (-0.5) * LOG2E

    def slot(dz, du):
        return lax.rem(z + (dz + 4), 4) * 4 + lax.rem(u + (du + 4), 4)

    def plain(src, dst, ssem, rsem, axis, step=1, only=None):
        links.send(lambda: (src, dst, ssem, rsem), axis, step, only)

    barrier = pltpu.get_barrier_semaphore()
    for axis, step in [("core", 1)] + [(a, s) for a in ("u", "w", "z") for s in (1, -1)]:
        pl.semaphore_signal(barrier, inc=1, device_id=links.peer(axis, step), device_id_type=MESH)
    crossed = x != y

    @pl.when(jnp.logical_and(core == 1, crossed))
    def _():
        for other in (0, 1):
            pl.semaphore_signal(barrier, inc=1, device_id={"y": x, "core": other, "x": y}, device_id_type=MESH)

    pl.semaphore_wait(barrier, 7 + jnp.where(crossed, 1, 0))

    def trows(dw, c):
        return tbuf.at[window(NEAR.index(dw) * 128 + c * 64, 64), :]

    own_tokens = pltpu.make_async_copy(tok, trows(0, core), lsem.at[0])
    own_tokens.start()

    own_rows = window(chip * 256 + core * 128, 128)
    items = []
    column = 0
    for ref, width in ((wq1, QK), (wq2, QK), (wk1, QK), (wk2, QK), (wv, V)):
        cols = pl.ds(column, width)
        items.append((ref.at[:, pl.ds(0, width)], ref.at[:, pl.ds(width, width)], wbuf.at[own_rows, cols]))
        column += width
    items.append((wo.at[pl.ds(0, 256), :], wo.at[pl.ds(256, 256), :], obuf.at[:, window((chip * 2 + core) * 128, 128)]))
    stays = jnp.logical_and(core == 1, x == y)
    leaves = jnp.logical_not(stays)

    def hand_over(which):
        for i in which:
            even, odd, dst = items[i]
            k = core * 6 + i
            plain(odd, dst, sss.at[6 + i], srs.at[k], "odd", only=leaves)
            pl.when(stays)(lambda: pltpu.make_async_copy(odd, dst, srs.at[k]).start())
            plain(even, dst, sss.at[i], srs.at[k], "even", only=core == 1)
            pl.when(core == 0)(lambda: pltpu.make_async_copy(even, dst, srs.at[k]).start())

    hand_over(range(5))
    plain(tok, tbuf.at[window(core * 64, 64), :], tss.at[6], trs.at[6], "core")
    plain(tok, tbuf.at[window(NEAR.index(-1) * 128 + core * 64, 64), :], tss.at[core], trs.at[core], "w", 1)
    plain(tok, tbuf.at[window(NEAR.index(1) * 128 + core * 64, 64), :], tss.at[2 + core], trs.at[2 + core], "w", -1)
    hand_over([5])

    for c in (0, 1):
        column = 0
        for i, width in enumerate((QK, QK, QK, QK, V)):
            view = wbuf.at[window(place * 256 + c * 128, 128), pl.ds(column, width)]
            links.arrived(view, sss.at[i], srs.at[c * 6 + i])
            column += width

    def wpiece(dz, du, part, sub):
        start = slot(dz, du) * 256 + part * 128
        if sub is None:
            return wbuf.at[window(start, 128), :]
        return wbuf.at[window(start + sub * 64, 64), :]

    weights = TorusGather(links, wpiece, wss, wrs)
    weights.begin()

    links.arrived(trows(0, 1 - core), tss.at[6], trs.at[6])
    sibling = trows(0, 1 - core)
    plain(sibling, tbuf.at[window(NEAR.index(-1) * 128 + (1 - core) * 64, 64), :], tss.at[1 - core], trs.at[1 - core], "w", 1)
    plain(sibling, tbuf.at[window(NEAR.index(1) * 128 + (1 - core) * 64, 64), :], tss.at[3 - core], trs.at[3 - core], "w", -1)

    lown[...] = jnp.full((8, 128), jnp.where(core == 0, lam[0], lam[1]), F32)

    def pass_on(dw, c, k, step):
        links.send(lambda: (trows(dw, c), trows(2, c), tss.at[k], trs.at[k]), "w", step)

    def near_tokens():
        for c in (0, 1):
            links.arrived(trows(-1, c), tss.at[c], trs.at[c])
        pass_on(-1, 0, 4, 1)
        for c in (0, 1):
            links.arrived(trows(1, c), tss.at[2 + c], trs.at[2 + c])
        pass_on(1, 1, 5, -1)
        own_tokens.wait()

    def far_tokens():
        for c in (0, 1):
            links.arrived(trows(2, c), tss.at[4 + c], trs.at[4 + c])

    def positions(ids, at_u):
        rel = ids // 128
        step = jnp.where(rel == 1, 3, jnp.where(rel == 2, 1, jnp.where(rel == 3, 2, 0)))
        along = (w + step) & 3
        return z * 2048 + at_u * (512 - 448 * core) + along * (64 + 448 * core) + ((ids // 64) & 1) * 256 + (ids & 63)

    half_dim = QK // 2
    position = positions(lax.broadcasted_iota(jnp.int32, (ROWS, half_dim), 0), u)
    angle = position.astype(F32) * inverse[...]
    cos_part, sin_part = jnp.cos(angle), jnp.sin(angle)
    cos[:, :half_dim] = cos_part
    cos[:, half_dim:] = cos_part
    sin[:, :half_dim] = -sin_part
    sin[:, half_dim:] = sin_part
    proj[...] = jnp.zeros_like(proj)

    steps = weights.steps()
    early = [action for actions, _ in steps[:8] for action in actions] + [near_tokens]
    dzs = [0] + [d for _, (d, _) in steps]
    dus = [0] + [d for _, (_, d) in steps]

    @pl.loop(0, 16)
    def _(t):
        on_step(t, 0, early)
        on_step(t, 5, [lambda: weights.third(0), lambda: weights.second(2, -1), lambda: weights.second(2, 1)])
        on_step(t, 11, [lambda: weights.third(-1)])
        on_step(t, 13, [lambda: weights.third(1)])
        on_step(t, 15, [lambda: weights.third(2)])
        depth = window(slot(pick(t, dzs), pick(t, dus)) * 256, 256)
        proj[0:384, :] += dot(tbuf[0:384, depth], wbuf[depth, :])

    def opiece(dz, du, part, sub):
        cols = window(slot(dz, du) * 256, 256)
        start, size = ((0, 64), (64, 192))[part]
        if sub is None:
            return obuf.at[pl.ds(start, size), cols]
        return obuf.at[pl.ds(start + sub * (size // 2), size // 2), cols]

    for c in (0, 1):
        links.arrived(obuf.at[:, window((place * 2 + c) * 128, 128)], sss.at[5], srs.at[c * 6 + 5])
    columns = TorusGather(links, opiece, oss, ors)
    columns.begin()
    far_tokens()
    proj[384:512, :] = dot(tbuf[384:512, :], wbuf[...])

    def turned(i):
        v = proj[:, i * QK : (i + 1) * QK]
        swapped = jnp.concatenate([v[:, QK // 2 :], v[:, : QK // 2]], axis=1)
        return (v * cos[...] + swapped * sin[...]).astype(BF)

    own_keys = window(place * ROWS, ROWS)
    kvbuf[own_keys, 0:QK] = turned(2)
    kvbuf[own_keys, QK : 2 * QK] = turned(3)
    kvbuf[own_keys, 2 * QK :] = proj[:, 4 * QK :].astype(BF)

    def kpiece(dz, du, part, sub):
        start, size = ((0, 128), (128, 384))[part]
        base = slot(dz, du) * ROWS + start
        if sub is None:
            return kvbuf.at[pl.ds(pl.multiple_of(base, 128), size), :]
        return kvbuf.at[pl.ds(pl.multiple_of(base + sub * (size // 2), 64), size // 2), :]

    keys = TorusGather(links, kpiece, kss, krs)
    keys.begin()
    crosses = jnp.logical_and(core == 1, crossed)
    plain(lown, lrecv, xss.at[0], xrs.at[0], "odd", only=crosses)
    pl.when(jnp.logical_not(crosses))(lambda: pltpu.make_async_copy(lown, lrecv, xrs.at[0]).start())
    qbuf[0] = turned(0)
    qbuf[1] = turned(1)

    def attend(index, at_u, masked, opening):
        span = window(index * ROWS, ROWS)
        v = kvbuf[span, 2 * QK :]
        for r in range(2):
            rows = pl.ds(r * 256, 256)
            if masked:
                query_at = positions(r * 256 + lax.broadcasted_iota(jnp.int32, (256, ROWS), 0), u)
                key_at = positions(lax.broadcasted_iota(jnp.int32, (256, ROWS), 1), at_u)
                allowed = key_at <= query_at
            for a in range(2):
                s = dot(qbuf[a, rows], kvbuf[span, a * QK : (a + 1) * QK], (((1,), (1,)), ((), ())))
                if masked:
                    s = jnp.where(allowed, s, -1e30)
                parts = [s[:, k * 128 : (k + 1) * 128] for k in range(4)]
                high = jnp.maximum(jnp.maximum(parts[0], parts[1]), jnp.maximum(parts[2], parts[3]))
                high = jnp.max(high, axis=1, keepdims=True) * log_scale
                if opening:
                    new = high
                else:
                    old = top[a, rows][:, :1]
                    new = jnp.maximum(old, high)
                e = jnp.exp2(s * log_scale - new)
                total = (e[:, 0:128] + e[:, 128:256]) + (e[:, 256:384] + e[:, 384:512])
                weighted = dot(e.astype(BF), v)
                if opening:
                    tot[a, rows] = total
                    acc[a, rows] = weighted
                else:
                    fade = jnp.exp2(old - new)
                    tot[a, rows] = tot[a, rows] * fade + total
                    acc[a, rows] = acc[a, rows] * fade + weighted
                top[a, rows] = jnp.broadcast_to(new, (256, 128))

    attend(place, u, True, True)

    ksteps = keys.steps()
    csteps = columns.steps()

    @pl.loop(0, 15)
    def _(t):
        for k in range(15):
            on_step(t, k, csteps[k][0] + ksteps[k][0])
        at_z = lax.rem(z + pick(t, dzs[1:]) + 4, 4)
        at_u = lax.rem(u + pick(t, dus[1:]) + 4, 4)
        index = at_z * 4 + at_u
        before = jnp.logical_and(at_z == z, jnp.logical_and(core == 0, at_u < u))

        @pl.when(jnp.logical_or(at_z < z, before))
        def _():
            attend(index, at_u, False, False)

        @pl.when(jnp.logical_and(at_z == z, core == 1))
        def _():
            attend(index, at_u, True, False)

    links.arrived(lrecv, xss.at[0], xrs.at[0])
    o1 = acc[0] / jnp.sum(tot[0], axis=1, keepdims=True)
    o2 = acc[1] / jnp.sum(tot[1], axis=1, keepdims=True)
    mixed = o1 - lrecv[0:1, 0:1] * o2
    norm = lax.rsqrt(jnp.mean(mixed * mixed, axis=1, keepdims=True) + EPS_NORM)
    mine[...] = (mixed * norm * gain[...]).astype(BF)

    def partial(dw):
        start = NEAR.index(dw) * 128
        return dot(mine[start : start + 128, :], obuf[...])

    term = partial(2)
    fsend[0] = term[:64].astype(BF)
    plain(fsend.at[0], frecv.at[0], xss.at[1], xrs.at[1], "w", 1)
    fsend[1] = term[64:].astype(BF)
    plain(fsend.at[1], frecv.at[1], xss.at[2], xrs.at[2], "w", -1)
    term = partial(1)
    nsend[1, 1] = term[64:].astype(BF)
    plain(nsend.at[1, 1], nrecv.at[1, 1], xss.at[3], xrs.at[3], "w", 1)
    keep[0] = term[:64]
    term = partial(-1)
    nsend[0, 0] = term[:64].astype(BF)
    plain(nsend.at[0, 0], nrecv.at[0, 0], xss.at[4], xrs.at[4], "w", -1)
    keep[1] = term[64:]
    term = partial(0)
    sums[0] = term[:64]
    sums[1] = term[64:]
    links.arrived(frecv.at[0], xss.at[1], xrs.at[1])
    nsend[1, 0] = (keep[0] + frecv[0].astype(F32)).astype(BF)
    plain(nsend.at[1, 0], nrecv.at[1, 0], xss.at[5], xrs.at[5], "w", 1)
    links.arrived(frecv.at[1], xss.at[2], xrs.at[2])
    nsend[0, 1] = (keep[1] + frecv[1].astype(F32)).astype(BF)
    plain(nsend.at[0, 1], nrecv.at[0, 1], xss.at[6], xrs.at[6], "w", -1)
    links.arrived(nrecv.at[1, 1], xss.at[3], xrs.at[3])
    sums[1] += nrecv[1, 1].astype(F32)
    links.arrived(nrecv.at[0, 0], xss.at[4], xrs.at[4])
    sums[0] += nrecv[0, 0].astype(F32)
    links.arrived(nrecv.at[1, 0], xss.at[5], xrs.at[5])
    sums[0] += nrecv[1, 0].astype(F32)
    links.arrived(nrecv.at[0, 1], xss.at[6], xrs.at[6])
    sums[1] += nrecv[0, 1].astype(F32)
    osend[...] = sums[1 - core].astype(BF)
    plain(osend, orecv, xss.at[7], xrs.at[7], "core")
    links.arrived(orecv, xss.at[7], xrs.at[7])
    out[...] = (sums[core] + orecv[...].astype(F32)).astype(BF)
    links.drain()


def on_device(tokens, query_one, query_two, key_one, key_two, value_weight, out_weight, lambdas, head_gain):
    inverse = 1.0 / np.float32(ROPE_BASE) ** (np.arange(0, QK, 2, dtype=np.float32) / np.float32(QK))
    vm = pl.BlockSpec(memory_space=pltpu.VMEM)
    dma = pltpu.SemaphoreType.DMA
    return pl.pallas_call(
        layer_kernel,
        out_shape=jax.ShapeDtypeStruct((64, 4096), BF),
        in_specs=[vm] * 7 + [pl.BlockSpec(memory_space=pltpu.SMEM)] + [vm] * 2,
        out_specs=vm,
        scratch_shapes=[
            pltpu.VMEM((ROWS, QK), F32),
            pltpu.VMEM((ROWS, QK), F32),
            pltpu.VMEM((ROWS, 4096), BF),
            pltpu.VMEM((4096, 768), BF),
            pltpu.VMEM((ROWS, 768), F32),
            pltpu.VMEM((2, ROWS, QK), BF),
            pltpu.VMEM((8192, 512), BF),
            pltpu.VMEM((256, 4096), BF),
            pltpu.VMEM((2, ROWS, V), F32),
            pltpu.VMEM((2, ROWS, 128), F32),
            pltpu.VMEM((2, ROWS, 128), F32),
            pltpu.VMEM((2, 64, 4096), BF),
            pltpu.VMEM((2, 64, 4096), BF),
            pltpu.VMEM((2, 2, 64, 4096), BF),
            pltpu.VMEM((2, 2, 64, 4096), BF),
            pltpu.VMEM((2, 64, 4096), F32),
            pltpu.VMEM((2, 64, 4096), F32),
            pltpu.VMEM((64, 4096), BF),
            pltpu.VMEM((64, 4096), BF),
            pltpu.VMEM((ROWS, V), BF),
            pltpu.VMEM((8, 128), F32),
            pltpu.VMEM((8, 128), F32),
            dma((1,)),
            dma((40,)), dma((40,)),
            dma((40,)), dma((40,)),
            dma((40,)), dma((40,)),
            dma((7,)), dma((7,)),
            dma((12,)), dma((12,)),
            dma((8,)), dma((8,)),
        ],
        compiler_params=pltpu.CompilerParams(
            collective_id=0, has_side_effects=True, vmem_limit_bytes=62 * 1024 * 1024
        ),
    )(tokens, query_one, query_two, key_one, key_two, value_weight, out_weight, lambdas, head_gain[None], jnp.asarray(inverse[None], F32))


def solution(mesh):
    fine = Mesh(mesh.devices.reshape(4, 4, 2, 4), AXES)
    sp = ("z", "y", "core")
    in_specs = (
        P((*sp, "x"), None),
        P(sp, "x"),
        P(sp, "x"),
        P(sp, "x"),
        P(sp, "x"),
        P(sp, "x"),
        P("x", sp),
        P("x"),
        P(),
    )
    return jax.shard_map(on_device, mesh=fine, in_specs=in_specs, out_specs=P((*sp, "x"), None), check_vma=False)
```

```python
import jax
import jax.numpy as jnp
import numpy as np
from jax import lax
from jax.experimental import pallas as pl
from jax.experimental.pallas import tpu as pltpu
from jax.sharding import Mesh, PartitionSpec as P

QK = 128
V = 256
ROPE_BASE = 500000.0
EPS_NORM = 0.02
LOG2E = 1.4426950408889634
ROWS = 512
BF = jnp.bfloat16
F32 = jnp.float32
MESH = pl.DeviceIdType.MESH
AXES = ("z", "y", "core", "x")
NEAR = (0, -1, 1, 2)


def dot(a, b, dims=(((1,), (0,)), ((), ()))):
    return lax.dot_general(a, b, dims, preferred_element_type=F32)


class Links:
    def __init__(self):
        self.z, self.y, self.core, self.x = [lax.axis_index(a) for a in AXES]
        self.u = self.y * (1 - self.core) + self.x * self.core
        self.w = self.x * (1 - self.core) + self.y * self.core
        self.sent = []
        self.later = []

    def peer(self, axis, step):
        if axis == "core":
            return {"core": 1 - self.core}
        if axis == "even":
            return {"core": 0}
        if axis == "odd":
            return {"y": self.x, "core": 1, "x": lax.rem(2 * self.x - self.y + 4, 4)}
        if axis == "z":
            return {"z": lax.rem(self.z + (step + 4), 4)}
        along = self.core if axis == "u" else 1 - self.core
        return {"y": lax.rem(self.y + (4 + step * (1 - along)), 4), "x": lax.rem(self.x + (4 + step * along), 4)}

    def send(self, views, axis, step, only=None, noted=True):
        def copy():
            return pltpu.make_async_remote_copy(*views(), device_id=self.peer(axis, step), device_id_type=MESH)

        if only is None:
            copy().start()
        else:
            pl.when(only)(lambda: copy().start())
        if noted:
            self.sent.append((copy, only))

    def arrived(self, view, ssem, rsem):
        pltpu.make_async_remote_copy(view, view, ssem, rsem, device_id=self.peer("core", 1), device_id_type=MESH).wait_recv()

    def drain(self):
        for copy, only in self.sent:
            if only is None:
                copy().wait_send()
            else:
                pl.when(only)(lambda copy=copy: copy().wait_send())
        for view, ssem in self.later:
            pltpu.make_async_remote_copy(view, view, ssem, ssem, device_id=self.peer("core", 1), device_id_type=MESH).wait_send()


class TorusGather:
    def __init__(self, links, piece, ssem, rsem, all_sent):
        self.links, self.piece, self.ssem, self.rsem = links, piece, ssem, rsem
        links.later.append((all_sent, ssem.at[0]))

    def ref(self, part, dp, ds, sub=None):
        dz, du = (ds, dp) if part == 0 else (dp, ds)
        return self.piece(dz, du, part, sub)

    def axis(self, part, second):
        return ("u", "z")[part ^ second]

    def out(self, part, key, dp, ds, sub, second, step):
        k = part * 20 + key

        def views():
            view = self.ref(part, dp, ds, sub)
            return view, view, self.ssem.at[0], self.rsem.at[k]

        self.links.send(views, self.axis(part, second), step, noted=False)

    def wait(self, part, key, dp, ds, sub):
        k = part * 20 + key
        self.links.arrived(self.ref(part, dp, ds, sub), self.ssem.at[0], self.rsem.at[k])

    def spread(self, part, dp):
        i = NEAR.index(dp)
        self.out(part, 4 + 4 * i, dp, 0, None, 1, 1)
        self.out(part, 5 + 4 * i, dp, 0, None, 1, -1)

    def begin(self):
        for part in (0, 1):
            self.out(part, 0, 0, 0, None, 0, 1)
            self.out(part, 1, 0, 0, None, 0, -1)
        for part in (0, 1):
            self.spread(part, 0)

    def first(self):
        for part in (0, 1):
            self.wait(part, 0, -1, 0, None)
            self.out(part, 2, -1, 0, 0, 0, 1)
            self.wait(part, 1, 1, 0, None)
            self.out(part, 3, 1, 0, 1, 0, -1)
        for part in (0, 1):
            self.spread(part, -1)
            self.spread(part, 1)

    def opposite(self):
        for part in (0, 1):
            self.wait(part, 2, 2, 0, 0)
            self.wait(part, 3, 2, 0, 1)
            self.spread(part, 2)

    def second(self, dp, step):
        i = NEAR.index(dp)
        for part in (0, 1):
            if step < 0:
                self.wait(part, 4 + 4 * i, dp, -1, None)
                self.out(part, 6 + 4 * i, dp, -1, 0, 1, 1)
            else:
                self.wait(part, 5 + 4 * i, dp, 1, None)
                self.out(part, 7 + 4 * i, dp, 1, 1, 1, -1)

    def third(self, dp):
        i = NEAR.index(dp)
        for part in (0, 1):
            self.wait(part, 6 + 4 * i, dp, 2, 0)
            self.wait(part, 7 + 4 * i, dp, 2, 1)

    def steps(self):
        second, third = self.second, self.third
        return [
            ([self.first, lambda: second(0, -1)], (-1, 0)),
            ([], (0, -1)),
            ([lambda: second(0, 1)], (1, 0)),
            ([], (0, 1)),
            ([self.opposite, lambda: second(-1, -1)], (-1, -1)),
            ([lambda: second(-1, 1), lambda: second(1, -1)], (1, -1)),
            ([], (-1, 1)),
            ([lambda: second(1, 1)], (1, 1)),
            ([lambda: third(0)], (0, 2)),
            ([], (2, 0)),
            ([lambda: second(2, -1), lambda: second(2, 1), lambda: third(-1)], (-1, 2)),
            ([], (2, -1)),
            ([lambda: third(1)], (1, 2)),
            ([], (2, 1)),
            ([lambda: third(2)], (2, 2)),
        ]


def pick(t, values):
    result = values[0]
    for k in range(1, len(values)):
        result = jnp.where(t == k, values[k], result)
    return result


def on_step(t, k, actions):
    if actions:

        @pl.when(t == k)
        def _():
            for action in actions:
                action()


def window(start, size):
    return pl.ds(pl.multiple_of(start, size), size)


def layer_kernel(
    tok, wq1, wq2, wk1, wk2, wv, wo, lam, gain, inverse, out, cos, sin,
    tbuf, wbuf, proj, qbuf, kvbuf, obuf, acc, top, tot,
    fsend, frecv, nsend, nrecv, keep, sums, osend, orecv, mine, lown, lrecv,
    lsem, wss, wrs, kss, krs, oss, ors, tss, trs, sss, srs, xss, xrs,
):
    links = Links()
    z, y, core, x, u, w = links.z, links.y, links.core, links.x, links.u, links.w
    other = 1 - core
    chip = z * 4 + y
    place = z * 4 + u
    log_scale = QK ** (-0.5) * LOG2E

    def slot(dz, du):
        return lax.rem(z + (dz + 4), 4) * 4 + lax.rem(u + (du + 4), 4)

    def depth_of(at_z, at_u):
        return at_z * 4 + jnp.where(core == 0, at_u, lax.rem(2 * w - at_u + 4, 4))

    def near_depth(dz, du):
        return depth_of(lax.rem(z + (dz + 4), 4), lax.rem(u + (du + 4), 4))

    own_depth = depth_of(z, u)

    def plain(src, dst, ssem, rsem, axis, step=1, only=None):
        links.send(lambda: (src, dst, ssem, rsem), axis, step, only)

    barrier = pltpu.get_barrier_semaphore()
    for axis, step in [("core", 1)] + [(a, s) for a in ("u", "w", "z") for s in (1, -1)]:
        pl.semaphore_signal(barrier, inc=1, device_id=links.peer(axis, step), device_id_type=MESH)
    crossed = x != y

    @pl.when(jnp.logical_and(core == 1, crossed))
    def _():
        for c in (0, 1):
            source = {"y": lax.rem(2 * y - x + 4, 4), "core": c, "x": y}
            pl.semaphore_signal(barrier, inc=1, device_id=source, device_id_type=MESH)

    pl.semaphore_wait(barrier, 7 + jnp.where(crossed, 1, 0))

    def trows(dw, c):
        return tbuf.at[window(NEAR.index(dw) * 128 + c * 64, 64), :]

    own_tokens = pltpu.make_async_copy(tok, trows(0, core), lsem.at[0])
    own_tokens.start()

    own_rows = window(chip * 256 + core * 128, 128)
    items = []
    column = 0
    for ref, width in ((wq1, QK), (wq2, QK), (wk1, QK), (wk2, QK), (wv, V)):
        cols = pl.ds(column, width)
        items.append((ref.at[:, pl.ds(0, width)], ref.at[:, pl.ds(width, width)], wbuf.at[own_rows, cols]))
        column += width
    items.append((wo.at[pl.ds(0, 256), :], wo.at[pl.ds(256, 256), :], obuf.at[:, window((chip * 2 + core) * 128, 128)]))
    stays = jnp.logical_and(core == 1, x == y)
    leaves = jnp.logical_not(stays)

    def hand_over(which):
        for i in which:
            even, odd, dst = items[i]
            k = core * 6 + i
            plain(odd, dst, sss.at[6 + i], srs.at[k], "odd", only=leaves)
            pl.when(stays)(lambda: pltpu.make_async_copy(odd, dst, srs.at[k]).start())
            plain(even, dst, sss.at[i], srs.at[k], "even", only=core == 1)
            pl.when(core == 0)(lambda: pltpu.make_async_copy(even, dst, srs.at[k]).start())

    hand_over(range(5))
    plain(tok, tbuf.at[window(core * 64, 64), :], tss.at[6], trs.at[6], "core")
    plain(tok, tbuf.at[window(NEAR.index(-1) * 128 + core * 64, 64), :], tss.at[core], trs.at[core], "w", 1)
    hand_over([5])

    for c in (0, 1):
        column = 0
        for i, width in enumerate((QK, QK, QK, QK, V)):
            view = wbuf.at[window(own_depth * 256 + c * 128, 128), pl.ds(column, width)]
            links.arrived(view, sss.at[i], srs.at[c * 6 + i])
            column += width

    def wpiece(dz, du, part, sub):
        start = near_depth(dz, du) * 256 + part * 128
        if sub is None:
            return wbuf.at[window(start, 128), :]
        return wbuf.at[window(start + sub * 64, 64), :]

    weights = TorusGather(links, wpiece, wss, wrs, wbuf.at[pl.ds(0, 3840), :])
    weights.begin()

    links.arrived(trows(0, other), tss.at[6], trs.at[6])
    sibling = trows(0, other)
    plain(sibling, tbuf.at[window(NEAR.index(1) * 128 + other * 64, 64), :], tss.at[2 + other], trs.at[2 + other], "w", -1)
    plain(tok, tbuf.at[window(NEAR.index(1) * 128 + core * 64, 64), :], tss.at[2 + core], trs.at[2 + core], "w", -1)
    plain(sibling, tbuf.at[window(NEAR.index(-1) * 128 + other * 64, 64), :], tss.at[other], trs.at[other], "w", 1)

    lown[...] = jnp.full((8, 128), jnp.where(core == 0, lam[0], lam[1]), F32)

    def pass_on(dw, c, k, step):
        links.send(lambda: (trows(dw, c), trows(2, c), tss.at[k], trs.at[k]), "w", step)

    def near_tokens():
        links.arrived(trows(-1, core), tss.at[core], trs.at[core])
        pass_on(-1, core, 4, 1)
        links.arrived(trows(1, other), tss.at[2 + other], trs.at[2 + other])
        pass_on(1, other, 5, -1)

    def near_tokens_rest():
        links.arrived(trows(-1, other), tss.at[other], trs.at[other])
        links.arrived(trows(1, core), tss.at[2 + core], trs.at[2 + core])
        own_tokens.wait()

    def far_tokens():
        links.arrived(trows(2, core), tss.at[4], trs.at[4])
        links.arrived(trows(2, other), tss.at[5], trs.at[5])

    def positions(ids, at_u):
        rel = ids // 128
        step = jnp.where(rel == 1, 3, jnp.where(rel == 2, 1, jnp.where(rel == 3, 2, 0)))
        along = (w + step) & 3
        return z * 2048 + at_u * (512 - 448 * core) + along * (64 + 448 * core) + ((ids // 64) & 1) * 256 + (ids & 63)

    half_dim = QK // 2
    position = positions(lax.broadcasted_iota(jnp.int32, (ROWS, half_dim), 0), u)
    angle = position.astype(F32) * inverse[...]
    cos_part, sin_part = jnp.cos(angle), jnp.sin(angle)
    cos[:, :half_dim] = cos_part
    cos[:, half_dim:] = cos_part
    sin[:, :half_dim] = -sin_part
    sin[:, half_dim:] = sin_part
    proj[...] = jnp.zeros_like(proj)

    steps = weights.steps()
    early = [action for actions, _ in steps[:6] for action in actions] + [near_tokens]
    early += [action for actions, _ in steps[6:8] for action in actions] + [near_tokens_rest]
    dzs = [0] + [d for _, (d, _) in steps]
    dus = [0] + [d for _, (_, d) in steps]

    @pl.loop(0, 16)
    def _(t):
        on_step(t, 0, early)
        on_step(t, 5, [lambda: weights.third(0), lambda: weights.second(2, -1), lambda: weights.second(2, 1)])
        on_step(t, 11, [lambda: weights.third(-1)])
        on_step(t, 13, [lambda: weights.third(1)])
        on_step(t, 15, [lambda: weights.third(2)])
        depth = window(near_depth(pick(t, dzs), pick(t, dus)) * 256, 256)
        proj[0:384, :] += dot(tbuf[0:384, depth], wbuf[depth, :])

    def opiece(dz, du, part, sub):
        cols = window(near_depth(dz, du) * 256, 256)
        start, size = ((0, 64), (64, 192))[part]
        if sub is None:
            return obuf.at[pl.ds(start, size), cols]
        return obuf.at[pl.ds(start + sub * (size // 2), size // 2), cols]

    for c in (0, 1):
        links.arrived(obuf.at[:, window((own_depth * 2 + c) * 128, 128)], sss.at[5], srs.at[c * 6 + 5])
    columns = TorusGather(links, opiece, oss, ors, obuf.at[:, pl.ds(0, 3840)])
    columns.begin()
    far_tokens()
    proj[384:512, :] = dot(tbuf[384:512, :], wbuf[...])

    def turned(i):
        v = proj[:, i * QK : (i + 1) * QK]
        swapped = jnp.concatenate([v[:, QK // 2 :], v[:, : QK // 2]], axis=1)
        return (v * cos[...] + swapped * sin[...]).astype(BF)

    own_keys = window(place * ROWS, ROWS)
    kvbuf[own_keys, 0:QK] = turned(2)
    kvbuf[own_keys, QK : 2 * QK] = turned(3)
    kvbuf[own_keys, 2 * QK :] = proj[:, 4 * QK :].astype(BF)

    def kpiece(dz, du, part, sub):
        start, size = ((0, 128), (128, 384))[part]
        base = slot(dz, du) * ROWS + start
        if sub is None:
            return kvbuf.at[pl.ds(pl.multiple_of(base, 128), size), :]
        return kvbuf.at[pl.ds(pl.multiple_of(base + sub * (size // 2), 64), size // 2), :]

    keys = TorusGather(links, kpiece, kss, krs, kvbuf.at[pl.ds(0, 7680), :])
    keys.begin()
    crosses = jnp.logical_and(core == 1, crossed)
    plain(lown, lrecv, xss.at[0], xrs.at[0], "odd", only=crosses)
    pl.when(jnp.logical_not(crosses))(lambda: pltpu.make_async_copy(lown, lrecv, xrs.at[0]).start())
    qbuf[0] = turned(0)
    qbuf[1] = turned(1)

    def attend(index, at_u, masked, opening):
        span = window(index * ROWS, ROWS)
        v = kvbuf[span, 2 * QK :]
        for r in range(2):
            rows = pl.ds(r * 256, 256)
            if masked:
                query_at = positions(r * 256 + lax.broadcasted_iota(jnp.int32, (256, ROWS), 0), u)
                key_at = positions(lax.broadcasted_iota(jnp.int32, (256, ROWS), 1), at_u)
                allowed = key_at <= query_at
            for a in range(2):
                s = dot(qbuf[a, rows], kvbuf[span, a * QK : (a + 1) * QK], (((1,), (1,)), ((), ())))
                if masked:
                    s = jnp.where(allowed, s, -1e30)
                parts = [s[:, k * 128 : (k + 1) * 128] for k in range(4)]
                high = jnp.maximum(jnp.maximum(parts[0], parts[1]), jnp.maximum(parts[2], parts[3]))
                high = jnp.max(high, axis=1, keepdims=True) * log_scale
                if opening:
                    new = high
                else:
                    old = top[a, rows][:, :1]
                    new = jnp.maximum(old, high)
                e = jnp.exp2(s * log_scale - new)
                total = (e[:, 0:128] + e[:, 128:256]) + (e[:, 256:384] + e[:, 384:512])
                weighted = dot(e.astype(BF), v)
                if opening:
                    tot[a, rows] = total
                    acc[a, rows] = weighted
                else:
                    fade = jnp.exp2(old - new)
                    tot[a, rows] = tot[a, rows] * fade + total
                    acc[a, rows] = acc[a, rows] * fade + weighted
                top[a, rows] = jnp.broadcast_to(new, (256, 128))

    attend(place, u, True, True)

    ksteps = keys.steps()
    csteps = columns.steps()

    @pl.loop(0, 15)
    def _(t):
        for k in range(15):
            on_step(t, k, csteps[k][0] + ksteps[k][0])
        at_z = lax.rem(z + pick(t, dzs[1:]) + 4, 4)
        at_u = lax.rem(u + pick(t, dus[1:]) + 4, 4)
        index = at_z * 4 + at_u
        before = jnp.logical_and(at_z == z, jnp.logical_and(core == 0, at_u < u))

        @pl.when(jnp.logical_or(at_z < z, before))
        def _():
            attend(index, at_u, False, False)

        @pl.when(jnp.logical_and(at_z == z, core == 1))
        def _():
            attend(index, at_u, True, False)

    links.arrived(lrecv, xss.at[0], xrs.at[0])
    o1 = acc[0] / jnp.sum(tot[0], axis=1, keepdims=True)
    o2 = acc[1] / jnp.sum(tot[1], axis=1, keepdims=True)
    mixed = o1 - lrecv[0:1, 0:1] * o2
    norm = lax.rsqrt(jnp.mean(mixed * mixed, axis=1, keepdims=True) + EPS_NORM)
    mine[...] = (mixed * norm * gain[...]).astype(BF)

    def partial(dw):
        start = NEAR.index(dw) * 128
        return dot(mine[start : start + 128, :], obuf[...])

    term = partial(2)
    fsend[0] = term[:64].astype(BF)
    plain(fsend.at[0], frecv.at[0], xss.at[1], xrs.at[1], "w", 1)
    fsend[1] = term[64:].astype(BF)
    plain(fsend.at[1], frecv.at[1], xss.at[2], xrs.at[2], "w", -1)
    term = partial(1)
    nsend[1, 1] = term[64:].astype(BF)
    plain(nsend.at[1, 1], nrecv.at[1, 1], xss.at[3], xrs.at[3], "w", 1)
    keep[0] = term[:64]
    term = partial(-1)
    nsend[0, 0] = term[:64].astype(BF)
    plain(nsend.at[0, 0], nrecv.at[0, 0], xss.at[4], xrs.at[4], "w", -1)
    keep[1] = term[64:]
    term = partial(0)
    sums[0] = term[:64]
    sums[1] = term[64:]
    links.arrived(frecv.at[0], xss.at[1], xrs.at[1])
    nsend[1, 0] = (keep[0] + frecv[0].astype(F32)).astype(BF)
    plain(nsend.at[1, 0], nrecv.at[1, 0], xss.at[5], xrs.at[5], "w", 1)
    links.arrived(frecv.at[1], xss.at[2], xrs.at[2])
    nsend[0, 1] = (keep[1] + frecv[1].astype(F32)).astype(BF)
    plain(nsend.at[0, 1], nrecv.at[0, 1], xss.at[6], xrs.at[6], "w", -1)
    links.arrived(nrecv.at[1, 1], xss.at[3], xrs.at[3])
    sums[1] += nrecv[1, 1].astype(F32)
    links.arrived(nrecv.at[0, 0], xss.at[4], xrs.at[4])
    sums[0] += nrecv[0, 0].astype(F32)
    links.arrived(nrecv.at[1, 0], xss.at[5], xrs.at[5])
    sums[0] += nrecv[1, 0].astype(F32)
    links.arrived(nrecv.at[0, 1], xss.at[6], xrs.at[6])
    sums[1] += nrecv[0, 1].astype(F32)
    osend[...] = sums[other].astype(BF)
    plain(osend, orecv, xss.at[7], xrs.at[7], "core")
    links.arrived(orecv, xss.at[7], xrs.at[7])
    out[...] = (sums[core] + orecv[...].astype(F32)).astype(BF)
    links.drain()


def on_device(tokens, query_one, query_two, key_one, key_two, value_weight, out_weight, lambdas, head_gain):
    inverse = 1.0 / np.float32(ROPE_BASE) ** (np.arange(0, QK, 2, dtype=np.float32) / np.float32(QK))
    vm = pl.BlockSpec(memory_space=pltpu.VMEM)
    dma = pltpu.SemaphoreType.DMA
    return pl.pallas_call(
        layer_kernel,
        out_shape=jax.ShapeDtypeStruct((64, 4096), BF),
        in_specs=[vm] * 7 + [pl.BlockSpec(memory_space=pltpu.SMEM)] + [vm] * 2,
        out_specs=vm,
        scratch_shapes=[
            pltpu.VMEM((ROWS, QK), F32),
            pltpu.VMEM((ROWS, QK), F32),
            pltpu.VMEM((ROWS, 4096), BF),
            pltpu.VMEM((4096, 768), BF),
            pltpu.VMEM((ROWS, 768), F32),
            pltpu.VMEM((2, ROWS, QK), BF),
            pltpu.VMEM((8192, 512), BF),
            pltpu.VMEM((256, 4096), BF),
            pltpu.VMEM((2, ROWS, V), F32),
            pltpu.VMEM((2, ROWS, 128), F32),
            pltpu.VMEM((2, ROWS, 128), F32),
            pltpu.VMEM((2, 64, 4096), BF),
            pltpu.VMEM((2, 64, 4096), BF),
            pltpu.VMEM((2, 2, 64, 4096), BF),
            pltpu.VMEM((2, 2, 64, 4096), BF),
            pltpu.VMEM((2, 64, 4096), F32),
            pltpu.VMEM((2, 64, 4096), F32),
            pltpu.VMEM((64, 4096), BF),
            pltpu.VMEM((64, 4096), BF),
            pltpu.VMEM((ROWS, V), BF),
            pltpu.VMEM((8, 128), F32),
            pltpu.VMEM((8, 128), F32),
            dma((1,)),
            dma((1,)), dma((40,)),
            dma((1,)), dma((40,)),
            dma((1,)), dma((40,)),
            dma((7,)), dma((7,)),
            dma((12,)), dma((12,)),
            dma((8,)), dma((8,)),
        ],
        compiler_params=pltpu.CompilerParams(
            collective_id=0, has_side_effects=True, vmem_limit_bytes=62 * 1024 * 1024
        ),
    )(tokens, query_one, query_two, key_one, key_two, value_weight, out_weight, lambdas, head_gain[None], jnp.asarray(inverse[None], F32))


def solution(mesh):
    fine = Mesh(mesh.devices.reshape(4, 4, 2, 4), AXES)
    sp = ("z", "y", "core")
    in_specs = (
        P((*sp, "x"), None),
        P(sp, "x"),
        P(sp, "x"),
        P(sp, "x"),
        P(sp, "x"),
        P(sp, "x"),
        P("x", sp),
        P("x"),
        P(),
    )
    return jax.shard_map(on_device, mesh=fine, in_specs=in_specs, out_specs=P((*sp, "x"), None), check_vma=False)
```

```python
import jax
import jax.numpy as jnp
import numpy as np
from jax import lax
from jax.experimental import pallas as pl
from jax.experimental.pallas import tpu as pltpu
from jax.sharding import Mesh, PartitionSpec as P

QK = 128
V = 256
ROPE_BASE = 500000.0
EPS_NORM = 0.02
LOG2E = 1.4426950408889634
ROWS = 512
BF = jnp.bfloat16
F32 = jnp.float32
MESH = pl.DeviceIdType.MESH
AXES = ("z", "y", "core", "x")
NEAR = (0, -1, 1, 2)


def dot(a, b, dims=(((1,), (0,)), ((), ()))):
    return lax.dot_general(a, b, dims, preferred_element_type=F32)


class Links:
    def __init__(self):
        self.z, self.y, self.core, self.x = [lax.axis_index(a) for a in AXES]
        self.u = self.y * (1 - self.core) + self.x * self.core
        self.w = self.x * (1 - self.core) + self.y * self.core
        self.sent = []
        self.later = []

    def peer(self, axis, step):
        if axis == "core":
            return {"core": 1 - self.core}
        if axis == "even":
            return {"core": 0}
        if axis == "turned":
            return {"y": self.x, "core": 0, "x": self.y}
        if axis == "odd":
            return {"y": self.x, "core": 1, "x": lax.rem(2 * self.x - self.y + 4, 4)}
        if axis == "z":
            return {"z": lax.rem(self.z + (step + 4), 4)}
        along = self.core if axis == "u" else 1 - self.core
        return {"y": lax.rem(self.y + (4 + step * (1 - along)), 4), "x": lax.rem(self.x + (4 + step * along), 4)}

    def send(self, views, axis, step, only=None, noted=True):
        def copy():
            return pltpu.make_async_remote_copy(*views(), device_id=self.peer(axis, step), device_id_type=MESH)

        if only is None:
            copy().start()
        else:
            pl.when(only)(lambda: copy().start())
        if noted:
            self.sent.append((copy, only))

    def arrived(self, view, ssem, rsem):
        pltpu.make_async_remote_copy(view, view, ssem, rsem, device_id=self.peer("core", 1), device_id_type=MESH).wait_recv()

    def drain(self):
        for copy, only in self.sent:
            if only is None:
                copy().wait_send()
            else:
                pl.when(only)(lambda copy=copy: copy().wait_send())
        for view, ssem in self.later:
            pltpu.make_async_remote_copy(view, view, ssem, ssem, device_id=self.peer("core", 1), device_id_type=MESH).wait_send()


class TorusGather:
    def __init__(self, links, piece, ssem, rsem, all_sent):
        self.links, self.piece, self.ssem, self.rsem = links, piece, ssem, rsem
        links.later.append((all_sent, ssem.at[0]))

    def ref(self, part, dp, ds, sub=None):
        dz, du = (ds, dp) if part == 0 else (dp, ds)
        return self.piece(dz, du, part, sub)

    def axis(self, part, second):
        return ("u", "z")[part ^ second]

    def out(self, part, key, dp, ds, sub, second, step):
        k = part * 20 + key

        def views():
            view = self.ref(part, dp, ds, sub)
            return view, view, self.ssem.at[0], self.rsem.at[k]

        self.links.send(views, self.axis(part, second), step, noted=False)

    def wait(self, part, key, dp, ds, sub):
        k = part * 20 + key
        self.links.arrived(self.ref(part, dp, ds, sub), self.ssem.at[0], self.rsem.at[k])

    def spread(self, part, dp):
        i = NEAR.index(dp)
        self.out(part, 4 + 4 * i, dp, 0, None, 1, 1)
        self.out(part, 5 + 4 * i, dp, 0, None, 1, -1)

    def begin(self):
        for part in (0, 1):
            self.out(part, 0, 0, 0, None, 0, 1)
            self.out(part, 1, 0, 0, None, 0, -1)
        for part in (0, 1):
            self.spread(part, 0)

    def first(self):
        for part in (0, 1):
            self.wait(part, 0, -1, 0, None)
            self.out(part, 2, -1, 0, 0, 0, 1)
            self.wait(part, 1, 1, 0, None)
            self.out(part, 3, 1, 0, 1, 0, -1)
        for part in (0, 1):
            self.spread(part, -1)
            self.spread(part, 1)

    def opposite(self):
        for part in (0, 1):
            self.wait(part, 2, 2, 0, 0)
            self.wait(part, 3, 2, 0, 1)
            self.spread(part, 2)

    def second(self, dp, step):
        i = NEAR.index(dp)
        for part in (0, 1):
            if step < 0:
                self.wait(part, 4 + 4 * i, dp, -1, None)
                self.out(part, 6 + 4 * i, dp, -1, 0, 1, 1)
            else:
                self.wait(part, 5 + 4 * i, dp, 1, None)
                self.out(part, 7 + 4 * i, dp, 1, 1, 1, -1)

    def third(self, dp):
        i = NEAR.index(dp)
        for part in (0, 1):
            self.wait(part, 6 + 4 * i, dp, 2, 0)
            self.wait(part, 7 + 4 * i, dp, 2, 1)

    def steps(self):
        second, third = self.second, self.third
        return [
            ([self.first, lambda: second(0, -1)], (-1, 0)),
            ([], (0, -1)),
            ([lambda: second(0, 1)], (1, 0)),
            ([], (0, 1)),
            ([self.opposite, lambda: second(-1, -1)], (-1, -1)),
            ([lambda: second(-1, 1), lambda: second(1, -1)], (1, -1)),
            ([], (-1, 1)),
            ([lambda: second(1, 1)], (1, 1)),
            ([lambda: third(0)], (0, 2)),
            ([], (2, 0)),
            ([lambda: second(2, -1), lambda: second(2, 1), lambda: third(-1)], (-1, 2)),
            ([], (2, -1)),
            ([lambda: third(1)], (1, 2)),
            ([], (2, 1)),
            ([lambda: third(2)], (2, 2)),
        ]


def pick(t, values):
    result = values[0]
    for k in range(1, len(values)):
        result = jnp.where(t == k, values[k], result)
    return result


def on_step(t, k, actions):
    if actions:

        @pl.when(t == k)
        def _():
            for action in actions:
                action()


def window(start, size):
    return pl.ds(pl.multiple_of(start, size), size)


def layer_kernel(
    tok, wq1, wq2, wk1, wk2, wv, wo, lam, gain, inverse, out, cos, sin,
    tbuf, wbuf, proj, qbuf, kvbuf, obuf, acc, top, tot,
    abuf, osum, fsend, passing, nsend, fin, sib, lown, lrecv,
    lsem, wss, wrs, kss, krs, oss, ors, tss, trs, sss, srs, xss, xrs,
):
    links = Links()
    z, y, core, x, u, w = links.z, links.y, links.core, links.x, links.u, links.w
    other = 1 - core
    chip = z * 4 + y
    place = z * 4 + u
    log_scale = QK ** (-0.5) * LOG2E

    def slot(dz, du):
        return lax.rem(z + (dz + 4), 4) * 4 + lax.rem(u + (du + 4), 4)

    def depth_of(at_z, at_u):
        return at_z * 4 + jnp.where(core == 0, at_u, lax.rem(2 * w - at_u + 4, 4))

    def near_depth(dz, du):
        return depth_of(lax.rem(z + (dz + 4), 4), lax.rem(u + (du + 4), 4))

    own_depth = depth_of(z, u)

    def plain(src, dst, ssem, rsem, axis, step=1, only=None):
        links.send(lambda: (src, dst, ssem, rsem), axis, step, only)

    barrier = pltpu.get_barrier_semaphore()
    for axis, step in [("core", 1)] + [(a, s) for a in ("u", "w", "z") for s in (1, -1)]:
        pl.semaphore_signal(barrier, inc=1, device_id=links.peer(axis, step), device_id_type=MESH)
    crossed = x != y

    @pl.when(jnp.logical_and(core == 1, crossed))
    def _():
        for c in (0, 1):
            source = {"y": lax.rem(2 * y - x + 4, 4), "core": c, "x": y}
            pl.semaphore_signal(barrier, inc=1, device_id=source, device_id_type=MESH)

    @pl.when(jnp.logical_and(core == 0, crossed))
    def _():
        for c in (0, 1):
            pl.semaphore_signal(barrier, inc=1, device_id={"y": x, "core": c, "x": y}, device_id_type=MESH)

    pl.semaphore_wait(barrier, 7 + jnp.where(crossed, 2, 0))

    def trows(dw, c):
        return tbuf.at[window(NEAR.index(dw) * 128 + c * 64, 64), :]

    own_tokens = pltpu.make_async_copy(tok, trows(0, core), lsem.at[0])
    own_tokens.start()

    own_rows = window(chip * 256 + core * 128, 128)
    items = []
    column = 0
    for ref, width in ((wq1, QK), (wq2, QK), (wk1, QK), (wk2, QK), (wv, V)):
        cols = pl.ds(column, width)
        items.append((ref.at[:, pl.ds(0, width)], ref.at[:, pl.ds(width, width)], wbuf.at[own_rows, cols]))
        column += width
    stays = jnp.logical_and(core == 1, x == y)
    leaves = jnp.logical_not(stays)

    def hand_over(which):
        for i in which:
            even, odd, dst = items[i]
            k = core * 6 + i
            plain(odd, dst, sss.at[6 + i], srs.at[k], "odd", only=leaves)
            pl.when(stays)(lambda: pltpu.make_async_copy(odd, dst, srs.at[k]).start())
            plain(even, dst, sss.at[i], srs.at[k], "even", only=core == 1)
            pl.when(core == 0)(lambda: pltpu.make_async_copy(even, dst, srs.at[k]).start())

    def hand_over_out():
        dst = obuf.at[window(x * 256, 256), window(z * 256 + core * 128, 128)]
        even, odd = wo.at[pl.ds(0, 256), :], wo.at[pl.ds(256, 256), :]
        k = core * 6 + 5
        here = jnp.logical_and(core == 0, x == y)
        plain(even, dst, sss.at[5], srs.at[k], "turned", only=jnp.logical_not(here))
        pl.when(here)(lambda: pltpu.make_async_copy(even, dst, srs.at[k]).start())
        plain(odd, dst, sss.at[11], srs.at[k], "core", only=core == 0)
        pl.when(core == 1)(lambda: pltpu.make_async_copy(odd, dst, srs.at[k]).start())

    hand_over(range(5))
    plain(tok, tbuf.at[window(core * 64, 64), :], tss.at[6], trs.at[6], "core")
    plain(tok, tbuf.at[window(NEAR.index(-1) * 128 + core * 64, 64), :], tss.at[core], trs.at[core], "w", 1)
    hand_over_out()

    for c in (0, 1):
        column = 0
        for i, width in enumerate((QK, QK, QK, QK, V)):
            view = wbuf.at[window(own_depth * 256 + c * 128, 128), pl.ds(column, width)]
            links.arrived(view, sss.at[i], srs.at[c * 6 + i])
            column += width

    def wpiece(dz, du, part, sub):
        start = near_depth(dz, du) * 256 + part * 128
        if sub is None:
            return wbuf.at[window(start, 128), :]
        return wbuf.at[window(start + sub * 64, 64), :]

    weights = TorusGather(links, wpiece, wss, wrs, wbuf.at[pl.ds(0, 3840), :])
    weights.begin()

    links.arrived(trows(0, other), tss.at[6], trs.at[6])
    sibling = trows(0, other)
    plain(sibling, tbuf.at[window(NEAR.index(1) * 128 + other * 64, 64), :], tss.at[2 + other], trs.at[2 + other], "w", -1)
    plain(tok, tbuf.at[window(NEAR.index(1) * 128 + core * 64, 64), :], tss.at[2 + core], trs.at[2 + core], "w", -1)
    plain(sibling, tbuf.at[window(NEAR.index(-1) * 128 + other * 64, 64), :], tss.at[other], trs.at[other], "w", 1)

    lown[...] = jnp.full((8, 128), jnp.where(core == 0, lam[0], lam[1]), F32)

    def pass_on(dw, c, k, step):
        links.send(lambda: (trows(dw, c), trows(2, c), tss.at[k], trs.at[k]), "w", step)

    def near_tokens():
        links.arrived(trows(-1, core), tss.at[core], trs.at[core])
        pass_on(-1, core, 4, 1)
        links.arrived(trows(1, other), tss.at[2 + other], trs.at[2 + other])
        pass_on(1, other, 5, -1)

    def near_tokens_rest():
        links.arrived(trows(-1, other), tss.at[other], trs.at[other])
        links.arrived(trows(1, core), tss.at[2 + core], trs.at[2 + core])
        own_tokens.wait()

    def far_tokens():
        links.arrived(trows(2, core), tss.at[4], trs.at[4])
        links.arrived(trows(2, other), tss.at[5], trs.at[5])

    def positions(ids, at_u):
        rel = ids // 128
        step = jnp.where(rel == 1, 3, jnp.where(rel == 2, 1, jnp.where(rel == 3, 2, 0)))
        along = (w + step) & 3
        return z * 2048 + at_u * (512 - 448 * core) + along * (64 + 448 * core) + ((ids // 64) & 1) * 256 + (ids & 63)

    half_dim = QK // 2
    position = positions(lax.broadcasted_iota(jnp.int32, (ROWS, half_dim), 0), u)
    angle = position.astype(F32) * inverse[...]
    cos_part, sin_part = jnp.cos(angle), jnp.sin(angle)
    cos[:, :half_dim] = cos_part
    cos[:, half_dim:] = cos_part
    sin[:, :half_dim] = -sin_part
    sin[:, half_dim:] = sin_part
    proj[...] = jnp.zeros_like(proj)

    steps = weights.steps()
    early = [action for actions, _ in steps[:6] for action in actions] + [near_tokens]
    early += [action for actions, _ in steps[6:8] for action in actions] + [near_tokens_rest]
    dzs = [0] + [d for _, (d, _) in steps]
    dus = [0] + [d for _, (_, d) in steps]

    @pl.loop(0, 16)
    def _(t):
        on_step(t, 0, early)
        on_step(t, 5, [lambda: weights.third(0), lambda: weights.second(2, -1), lambda: weights.second(2, 1)])
        on_step(t, 11, [lambda: weights.third(-1)])
        on_step(t, 13, [lambda: weights.third(1)])
        on_step(t, 15, [lambda: weights.third(2)])
        depth = window(near_depth(pick(t, dzs), pick(t, dus)) * 256, 256)
        proj[0:384, :] += dot(tbuf[0:384, depth], wbuf[depth, :])

    def opiece(dz, du, part, sub):
        cols = window(lax.rem(z + (dz + 4), 4) * 256, 256)
        start, size = ((0, 64), (64, 192))[part]
        base = lax.rem(u + (du + 4), 4) * 256 + start
        if sub is None:
            return obuf.at[pl.ds(pl.multiple_of(base, 64), size), cols]
        return obuf.at[pl.ds(pl.multiple_of(base + sub * (size // 2), 32), size // 2), cols]

    for c in (0, 1):
        links.arrived(obuf.at[window(u * 256, 256), window(z * 256 + c * 128, 128)], sss.at[5], srs.at[c * 6 + 5])
    columns = TorusGather(links, opiece, oss, ors, obuf.at[pl.ds(0, 960), :])
    columns.begin()
    far_tokens()
    proj[384:512, :] = dot(tbuf[384:512, :], wbuf[...])

    def turned(i):
        v = proj[:, i * QK : (i + 1) * QK]
        swapped = jnp.concatenate([v[:, QK // 2 :], v[:, : QK // 2]], axis=1)
        return (v * cos[...] + swapped * sin[...]).astype(BF)

    own_keys = window(place * ROWS, ROWS)
    kvbuf[own_keys, 0:QK] = turned(2)
    kvbuf[own_keys, QK : 2 * QK] = turned(3)
    kvbuf[own_keys, 2 * QK :] = proj[:, 4 * QK :].astype(BF)

    def kpiece(dz, du, part, sub):
        start, size = ((0, 128), (128, 384))[part]
        base = slot(dz, du) * ROWS + start
        if sub is None:
            return kvbuf.at[pl.ds(pl.multiple_of(base, 128), size), :]
        return kvbuf.at[pl.ds(pl.multiple_of(base + sub * (size // 2), 64), size // 2), :]

    keys = TorusGather(links, kpiece, kss, krs, kvbuf.at[pl.ds(0, 7680), :])
    keys.begin()
    crosses = jnp.logical_and(core == 1, crossed)
    plain(lown, lrecv, xss.at[0], xrs.at[0], "odd", only=crosses)
    pl.when(jnp.logical_not(crosses))(lambda: pltpu.make_async_copy(lown, lrecv, xrs.at[0]).start())
    qbuf[0] = turned(0)
    qbuf[1] = turned(1)

    def attend(index, at_u, masked, opening):
        span = window(index * ROWS, ROWS)
        v = kvbuf[span, 2 * QK :]
        for r in range(2):
            rows = pl.ds(r * 256, 256)
            if masked:
                query_at = positions(r * 256 + lax.broadcasted_iota(jnp.int32, (256, ROWS), 0), u)
                key_at = positions(lax.broadcasted_iota(jnp.int32, (256, ROWS), 1), at_u)
                allowed = key_at <= query_at
            for a in range(2):
                s = dot(qbuf[a, rows], kvbuf[span, a * QK : (a + 1) * QK], (((1,), (1,)), ((), ())))
                if masked:
                    s = jnp.where(allowed, s, -1e30)
                parts = [s[:, k * 128 : (k + 1) * 128] for k in range(4)]
                high = jnp.maximum(jnp.maximum(parts[0], parts[1]), jnp.maximum(parts[2], parts[3]))
                high = jnp.max(high, axis=1, keepdims=True) * log_scale
                if opening:
                    new = high
                else:
                    old = top[a, rows][:, :1]
                    new = jnp.maximum(old, high)
                e = jnp.exp2(s * log_scale - new)
                total = (e[:, 0:128] + e[:, 128:256]) + (e[:, 256:384] + e[:, 384:512])
                weighted = dot(e.astype(BF), v)
                if opening:
                    tot[a, rows] = total
                    acc[a, rows] = weighted
                else:
                    fade = jnp.exp2(old - new)
                    tot[a, rows] = tot[a, rows] * fade + total
                    acc[a, rows] = acc[a, rows] * fade + weighted
                top[a, rows] = jnp.broadcast_to(new, (256, 128))

    attend(place, u, True, True)

    ksteps = keys.steps()
    csteps = columns.steps()
    early_columns = [[] for _ in range(15)]
    for k in range(15):
        early_columns[max(k - 1, 0)] += csteps[k][0]

    @pl.loop(0, 15)
    def _(t):
        for k in range(15):
            on_step(t, k, early_columns[k] + ksteps[k][0])
        at_z = lax.rem(z + pick(t, dzs[1:]) + 4, 4)
        at_u = lax.rem(u + pick(t, dus[1:]) + 4, 4)
        index = at_z * 4 + at_u
        before = jnp.logical_and(at_z == z, jnp.logical_and(core == 0, at_u < u))

        @pl.when(jnp.logical_or(at_z < z, before))
        def _():
            attend(index, at_u, False, False)

        @pl.when(jnp.logical_and(at_z == z, core == 1))
        def _():
            attend(index, at_u, True, False)

    links.arrived(lrecv, xss.at[0], xrs.at[0])

    def finish(h):
        rows = pl.ds(h * 256, 256)
        o1 = acc[0, rows] / jnp.sum(tot[0, rows], axis=1, keepdims=True)
        o2 = acc[1, rows] / jnp.sum(tot[1, rows], axis=1, keepdims=True)
        mixed = o1 - lrecv[0:1, 0:1] * o2
        norm = lax.rsqrt(jnp.mean(mixed * mixed, axis=1, keepdims=True) + EPS_NORM)
        abuf[0, rows] = (mixed * norm * gain[...]).astype(BF)

    def heads(k, h):
        return abuf.at[k, pl.ds(h * 256, 256), :]

    def along(src, dst, k, step):
        plain(src, dst, xss.at[k], xrs.at[k], "w", step)

    def got(view, k):
        links.arrived(view, xss.at[k], xrs.at[k])

    seen = set()

    def add(dw, h):
        head = window(lax.rem(w + (dw + 4), 4) * 256, 256)
        term = dot(abuf[NEAR.index(dw), h * 256 : (h + 1) * 256, :], obuf[head, :])
        for b in (0, 1):
            target = (dw + NEAR[2 * h + b]) % 4
            j = NEAR.index(-1 if target == 3 else target)
            block = term[b * 128 : (b + 1) * 128]
            if j in seen:
                osum[j] += block
            else:
                osum[j] = block
            seen.add(j)

    finish(0)
    along(heads(0, 0), heads(1, 0), 1, 1)
    finish(1)
    along(heads(0, 1), heads(2, 1), 4, -1)
    along(heads(0, 0), heads(2, 0), 3, -1)
    along(heads(0, 1), heads(1, 1), 2, 1)
    add(0, 0)
    add(0, 1)
    got(heads(1, 0), 1)
    along(heads(1, 0), heads(3, 0), 5, 1)
    got(heads(2, 1), 4)
    along(heads(2, 1), heads(3, 1), 6, -1)
    add(-1, 0)
    add(1, 1)
    got(heads(1, 1), 2)
    add(-1, 1)
    got(heads(2, 0), 3)
    add(1, 0)
    got(heads(3, 0), 5)
    add(2, 0)
    got(heads(3, 1), 6)
    add(2, 1)

    for r, step in ((0, 1), (1, -1)):
        fsend[r] = osum[3, r * 64 : (r + 1) * 64].astype(BF)
        along(fsend.at[r], passing.at[r], 7 + r, step)
    nsend[0] = osum[2].astype(BF)
    along(nsend.at[0], fin.at[1], 9, 1)
    nsend[1] = osum[1].astype(BF)
    along(nsend.at[1], fin.at[2], 10, -1)
    fin[0] = osum[0].astype(BF)
    other_rows = window(other * 64, 64)

    def to_sibling(k):
        at_w = lax.rem(w + (NEAR[k] + 4), 4)
        plain(fin.at[k, other_rows, :], sib.at[at_w], xss.at[13 + k], xrs.at[13 + at_w], "core")

    to_sibling(0)
    for r, step in ((0, 1), (1, -1)):
        got(passing.at[r], 7 + r)
        along(passing.at[r], fin.at[3, pl.ds(r * 64, 64), :], 11 + r, step)
    got(fin.at[1], 9)
    to_sibling(1)
    got(fin.at[2], 10)
    to_sibling(2)
    got(fin.at[3, pl.ds(0, 64), :], 11)
    got(fin.at[3, pl.ds(64, 64), :], 12)
    to_sibling(3)
    own_part = window(core * 64, 64)
    for k in range(4):
        at_w = lax.rem(w + (NEAR[k] + 4), 4)
        links.arrived(sib.at[at_w], xss.at[13 + k], xrs.at[13 + at_w])
        both = (fin[k, own_part, :].astype(F32) + sib[at_w].astype(F32)).astype(BF)
        for c in range(4):
            out[:, window((c * 4 + at_w) * 256, 256)] = both[:, c * 256 : (c + 1) * 256]
    links.drain()


def on_device(tokens, query_one, query_two, key_one, key_two, value_weight, out_weight, lambdas, head_gain):
    inverse = 1.0 / np.float32(ROPE_BASE) ** (np.arange(0, QK, 2, dtype=np.float32) / np.float32(QK))
    vm = pl.BlockSpec(memory_space=pltpu.VMEM)
    dma = pltpu.SemaphoreType.DMA
    return pl.pallas_call(
        layer_kernel,
        out_shape=jax.ShapeDtypeStruct((64, 4096), BF),
        in_specs=[vm] * 7 + [pl.BlockSpec(memory_space=pltpu.SMEM)] + [vm] * 2,
        out_specs=vm,
        scratch_shapes=[
            pltpu.VMEM((ROWS, QK), F32),
            pltpu.VMEM((ROWS, QK), F32),
            pltpu.VMEM((ROWS, 4096), BF),
            pltpu.VMEM((4096, 768), BF),
            pltpu.VMEM((ROWS, 768), F32),
            pltpu.VMEM((2, ROWS, QK), BF),
            pltpu.VMEM((8192, 512), BF),
            pltpu.VMEM((1024, 1024), BF),
            pltpu.VMEM((2, ROWS, V), F32),
            pltpu.VMEM((2, ROWS, 128), F32),
            pltpu.VMEM((2, ROWS, 128), F32),
            pltpu.VMEM((4, ROWS, V), BF),
            pltpu.VMEM((4, 128, 1024), F32),
            pltpu.VMEM((2, 64, 1024), BF),
            pltpu.VMEM((2, 64, 1024), BF),
            pltpu.VMEM((2, 128, 1024), BF),
            pltpu.VMEM((4, 128, 1024), BF),
            pltpu.VMEM((4, 64, 1024), BF),
            pltpu.VMEM((8, 128), F32),
            pltpu.VMEM((8, 128), F32),
            dma((1,)),
            dma((1,)), dma((40,)),
            dma((1,)), dma((40,)),
            dma((1,)), dma((40,)),
            dma((7,)), dma((7,)),
            dma((12,)), dma((12,)),
            dma((17,)), dma((17,)),
        ],
        compiler_params=pltpu.CompilerParams(
            collective_id=0, has_side_effects=True, vmem_limit_bytes=62 * 1024 * 1024
        ),
    )(tokens, query_one, query_two, key_one, key_two, value_weight, out_weight, lambdas, head_gain[None], jnp.asarray(inverse[None], F32))


def solution(mesh):
    fine = Mesh(mesh.devices.reshape(4, 4, 2, 4), AXES)
    sp = ("z", "y", "core")
    in_specs = (
        P((*sp, "x"), None),
        P(sp, "x"),
        P(sp, "x"),
        P(sp, "x"),
        P(sp, "x"),
        P(sp, "x"),
        P("x", sp),
        P("x"),
        P(),
    )
    return jax.shard_map(on_device, mesh=fine, in_specs=in_specs, out_specs=P((*sp, "x"), None), check_vma=False)
```

```python
import jax
import jax.numpy as jnp
import numpy as np
from jax import lax
from jax.experimental import pallas as pl
from jax.experimental.pallas import tpu as pltpu
from jax.sharding import Mesh, PartitionSpec as P

QK = 128
V = 256
ROPE_BASE = 500000.0
EPS_NORM = 0.02
LOG2E = 1.4426950408889634
ROWS = 512
BF = jnp.bfloat16
F32 = jnp.float32
MESH = pl.DeviceIdType.MESH
AXES = ("z", "y", "core", "x")
NEAR = (0, -1, 1, 2)


def dot(a, b, dims=(((1,), (0,)), ((), ()))):
    return lax.dot_general(a, b, dims, preferred_element_type=F32)


class Links:
    def __init__(self):
        self.z, self.y, self.core, self.x = [lax.axis_index(a) for a in AXES]
        self.u = self.y * (1 - self.core) + self.x * self.core
        self.w = self.x * (1 - self.core) + self.y * self.core
        self.sent = []
        self.later = []

    def peer(self, axis, step):
        if axis == "core":
            return {"core": 1 - self.core}
        if axis == "even":
            return {"core": 0}
        if axis == "turned":
            return {"y": self.x, "core": 0, "x": self.y}
        if axis == "odd":
            return {"y": self.x, "core": 1, "x": lax.rem(2 * self.x - self.y + 4, 4)}
        if axis == "z":
            return {"z": lax.rem(self.z + (step + 4), 4)}
        along = self.core if axis == "u" else 1 - self.core
        return {"y": lax.rem(self.y + (4 + step * (1 - along)), 4), "x": lax.rem(self.x + (4 + step * along), 4)}

    def send(self, views, axis, step, only=None, noted=True):
        def copy():
            return pltpu.make_async_remote_copy(*views(), device_id=self.peer(axis, step), device_id_type=MESH)

        if only is None:
            copy().start()
        else:
            pl.when(only)(lambda: copy().start())
        if noted:
            self.sent.append((copy, only))

    def arrived(self, view, ssem, rsem):
        pltpu.make_async_remote_copy(view, view, ssem, rsem, device_id=self.peer("core", 1), device_id_type=MESH).wait_recv()

    def drain(self):
        for copy, only in self.sent:
            if only is None:
                copy().wait_send()
            else:
                pl.when(only)(lambda copy=copy: copy().wait_send())
        for view, ssem in self.later:
            pltpu.make_async_remote_copy(view, view, ssem, ssem, device_id=self.peer("core", 1), device_id_type=MESH).wait_send()


class TorusGather:
    def __init__(self, links, piece, ssem, rsem, all_sent):
        self.links, self.piece, self.ssem, self.rsem = links, piece, ssem, rsem
        links.later.append((all_sent, ssem.at[0]))

    def ref(self, part, dp, ds, sub=None):
        dz, du = (ds, dp) if part == 0 else (dp, ds)
        return self.piece(dz, du, part, sub)

    def axis(self, part, second):
        return ("u", "z")[part ^ second]

    def out(self, part, key, dp, ds, sub, second, step):
        k = part * 20 + key

        def views():
            view = self.ref(part, dp, ds, sub)
            return view, view, self.ssem.at[0], self.rsem.at[k]

        self.links.send(views, self.axis(part, second), step, noted=False)

    def wait(self, part, key, dp, ds, sub):
        k = part * 20 + key
        self.links.arrived(self.ref(part, dp, ds, sub), self.ssem.at[0], self.rsem.at[k])

    def spread(self, part, dp):
        i = NEAR.index(dp)
        self.out(part, 4 + 4 * i, dp, 0, None, 1, 1)
        self.out(part, 5 + 4 * i, dp, 0, None, 1, -1)

    def begin(self):
        for part in (0, 1):
            self.out(part, 0, 0, 0, None, 0, 1)
            self.out(part, 1, 0, 0, None, 0, -1)
        for part in (0, 1):
            self.spread(part, 0)

    def first(self):
        for part in (0, 1):
            self.wait(part, 0, -1, 0, None)
            self.out(part, 2, -1, 0, 0, 0, 1)
            self.wait(part, 1, 1, 0, None)
            self.out(part, 3, 1, 0, 1, 0, -1)
        for part in (0, 1):
            self.spread(part, -1)
            self.spread(part, 1)

    def opposite(self):
        for part in (0, 1):
            self.wait(part, 2, 2, 0, 0)
            self.wait(part, 3, 2, 0, 1)
            self.spread(part, 2)

    def second(self, dp, step):
        i = NEAR.index(dp)
        for part in (0, 1):
            if step < 0:
                self.wait(part, 4 + 4 * i, dp, -1, None)
                self.out(part, 6 + 4 * i, dp, -1, 0, 1, 1)
            else:
                self.wait(part, 5 + 4 * i, dp, 1, None)
                self.out(part, 7 + 4 * i, dp, 1, 1, 1, -1)

    def third(self, dp):
        i = NEAR.index(dp)
        for part in (0, 1):
            self.wait(part, 6 + 4 * i, dp, 2, 0)
            self.wait(part, 7 + 4 * i, dp, 2, 1)

    def steps(self):
        second, third = self.second, self.third
        return [
            ([self.first, lambda: second(0, -1)], (-1, 0)),
            ([], (0, -1)),
            ([lambda: second(0, 1)], (1, 0)),
            ([], (0, 1)),
            ([self.opposite, lambda: second(-1, -1)], (-1, -1)),
            ([lambda: second(-1, 1), lambda: second(1, -1)], (1, -1)),
            ([], (-1, 1)),
            ([lambda: second(1, 1)], (1, 1)),
            ([lambda: third(0)], (0, 2)),
            ([], (2, 0)),
            ([lambda: second(2, -1), lambda: second(2, 1), lambda: third(-1)], (-1, 2)),
            ([], (2, -1)),
            ([lambda: third(1)], (1, 2)),
            ([], (2, 1)),
            ([lambda: third(2)], (2, 2)),
        ]


def pick(t, values):
    result = values[0]
    for k in range(1, len(values)):
        result = jnp.where(t == k, values[k], result)
    return result


def on_step(t, k, actions):
    if actions:

        @pl.when(t == k)
        def _():
            for action in actions:
                action()


def window(start, size):
    return pl.ds(pl.multiple_of(start, size), size)


def layer_kernel(
    tok, wq1, wq2, wk1, wk2, wv, wo, lam, gain, inverse, out, cos, sin,
    tbuf, wbuf, proj, qbuf, kvbuf, obuf, acc, top, tot,
    abuf, osum, fsend, passing, nsend, fin, sib, lown, lrecv,
    lsem, wss, wrs, kss, krs, oss, ors, tss, trs, sss, srs, xss, xrs,
):
    links = Links()
    z, y, core, x, u, w = links.z, links.y, links.core, links.x, links.u, links.w
    other = 1 - core
    chip = z * 4 + y
    place = z * 4 + u
    log_scale = QK ** (-0.5) * LOG2E

    def slot(dz, du):
        return lax.rem(z + (dz + 4), 4) * 4 + lax.rem(u + (du + 4), 4)

    def depth_of(at_z, at_u):
        return at_z * 4 + jnp.where(core == 0, at_u, lax.rem(2 * w - at_u + 4, 4))

    def near_depth(dz, du):
        return depth_of(lax.rem(z + (dz + 4), 4), lax.rem(u + (du + 4), 4))

    own_depth = depth_of(z, u)

    def plain(src, dst, ssem, rsem, axis, step=1, only=None):
        links.send(lambda: (src, dst, ssem, rsem), axis, step, only)

    barrier = pltpu.get_barrier_semaphore()
    for axis, step in [("core", 1)] + [(a, s) for a in ("u", "w", "z") for s in (1, -1)]:
        pl.semaphore_signal(barrier, inc=1, device_id=links.peer(axis, step), device_id_type=MESH)
    crossed = x != y

    @pl.when(jnp.logical_and(core == 1, crossed))
    def _():
        for c in (0, 1):
            source = {"y": lax.rem(2 * y - x + 4, 4), "core": c, "x": y}
            pl.semaphore_signal(barrier, inc=1, device_id=source, device_id_type=MESH)

    @pl.when(jnp.logical_and(core == 0, crossed))
    def _():
        for c in (0, 1):
            pl.semaphore_signal(barrier, inc=1, device_id={"y": x, "core": c, "x": y}, device_id_type=MESH)

    pl.semaphore_wait(barrier, 7 + jnp.where(crossed, 2, 0))

    def trows(dw, c):
        return tbuf.at[window(NEAR.index(dw) * 128 + c * 64, 64), :]

    own_tokens = pltpu.make_async_copy(tok, trows(0, core), lsem.at[0])
    own_tokens.start()

    own_rows = window(chip * 256 + core * 128, 128)
    items = []
    column = 0
    for ref, width in ((wq1, QK), (wq2, QK), (wk1, QK), (wk2, QK), (wv, V)):
        cols = pl.ds(column, width)
        items.append((ref.at[:, pl.ds(0, width)], ref.at[:, pl.ds(width, width)], wbuf.at[own_rows, cols]))
        column += width
    stays = jnp.logical_and(core == 1, x == y)
    leaves = jnp.logical_not(stays)

    def hand_over(which):
        for i in which:
            even, odd, dst = items[i]
            k = core * 6 + i
            plain(odd, dst, sss.at[6 + i], srs.at[k], "odd", only=leaves)
            pl.when(stays)(lambda: pltpu.make_async_copy(odd, dst, srs.at[k]).start())
            plain(even, dst, sss.at[i], srs.at[k], "even", only=core == 1)
            pl.when(core == 0)(lambda: pltpu.make_async_copy(even, dst, srs.at[k]).start())

    def hand_over_out():
        dst = obuf.at[window(x * 256, 256), window(z * 256 + core * 128, 128)]
        even, odd = wo.at[pl.ds(0, 256), :], wo.at[pl.ds(256, 256), :]
        k = core * 6 + 5
        here = jnp.logical_and(core == 0, x == y)
        plain(even, dst, sss.at[5], srs.at[k], "turned", only=jnp.logical_not(here))
        pl.when(here)(lambda: pltpu.make_async_copy(even, dst, srs.at[k]).start())
        plain(odd, dst, sss.at[11], srs.at[k], "core", only=core == 0)
        pl.when(core == 1)(lambda: pltpu.make_async_copy(odd, dst, srs.at[k]).start())

    hand_over(range(5))
    plain(tok, tbuf.at[window(core * 64, 64), :], tss.at[6], trs.at[6], "core")
    plain(tok, tbuf.at[window(NEAR.index(-1) * 128 + core * 64, 64), :], tss.at[core], trs.at[core], "w", 1)
    hand_over_out()

    for c in (0, 1):
        column = 0
        for i, width in enumerate((QK, QK, QK, QK, V)):
            view = wbuf.at[window(own_depth * 256 + c * 128, 128), pl.ds(column, width)]
            links.arrived(view, sss.at[i], srs.at[c * 6 + i])
            column += width

    def wpiece(dz, du, part, sub):
        start = near_depth(dz, du) * 256 + part * 128
        if sub is None:
            return wbuf.at[window(start, 128), :]
        return wbuf.at[window(start + sub * 64, 64), :]

    weights = TorusGather(links, wpiece, wss, wrs, wbuf.at[pl.ds(0, 3840), :])
    weights.begin()

    links.arrived(trows(0, other), tss.at[6], trs.at[6])
    sibling = trows(0, other)
    plain(sibling, tbuf.at[window(NEAR.index(1) * 128 + other * 64, 64), :], tss.at[2 + other], trs.at[2 + other], "w", -1)
    plain(tok, tbuf.at[window(NEAR.index(1) * 128 + core * 64, 64), :], tss.at[2 + core], trs.at[2 + core], "w", -1)
    plain(sibling, tbuf.at[window(NEAR.index(-1) * 128 + other * 64, 64), :], tss.at[other], trs.at[other], "w", 1)

    lown[...] = jnp.full((8, 128), jnp.where(core == 0, lam[0], lam[1]), F32)

    def pass_on(dw, c, k, step):
        links.send(lambda: (trows(dw, c), trows(2, c), tss.at[k], trs.at[k]), "w", step)

    def near_tokens():
        links.arrived(trows(-1, core), tss.at[core], trs.at[core])
        pass_on(-1, core, 4, 1)
        links.arrived(trows(1, other), tss.at[2 + other], trs.at[2 + other])
        pass_on(1, other, 5, -1)

    def near_tokens_rest():
        links.arrived(trows(-1, other), tss.at[other], trs.at[other])
        links.arrived(trows(1, core), tss.at[2 + core], trs.at[2 + core])
        own_tokens.wait()

    def far_tokens():
        links.arrived(trows(2, core), tss.at[4], trs.at[4])
        links.arrived(trows(2, other), tss.at[5], trs.at[5])

    def positions(ids, at_u):
        rel = ids // 128
        step = jnp.where(rel == 1, 3, jnp.where(rel == 2, 1, jnp.where(rel == 3, 2, 0)))
        along = (w + step) & 3
        return z * 2048 + at_u * (512 - 448 * core) + along * (64 + 448 * core) + ((ids // 64) & 1) * 256 + (ids & 63)

    half_dim = QK // 2
    position = positions(lax.broadcasted_iota(jnp.int32, (ROWS, half_dim), 0), u)
    angle = position.astype(F32) * inverse[...]
    cos_part, sin_part = jnp.cos(angle), jnp.sin(angle)
    cos[:, :half_dim] = cos_part
    cos[:, half_dim:] = cos_part
    sin[:, :half_dim] = -sin_part
    sin[:, half_dim:] = sin_part
    proj[...] = jnp.zeros_like(proj)

    steps = weights.steps()
    early = [action for actions, _ in steps[:6] for action in actions] + [near_tokens]
    early += [action for actions, _ in steps[6:8] for action in actions] + [near_tokens_rest]
    dzs = [0] + [d for _, (d, _) in steps]
    dus = [0] + [d for _, (_, d) in steps]

    @pl.loop(0, 16)
    def _(t):
        on_step(t, 0, early)
        on_step(t, 5, [lambda: weights.third(0), lambda: weights.second(2, -1), lambda: weights.second(2, 1)])
        on_step(t, 11, [lambda: weights.third(-1)])
        on_step(t, 13, [lambda: weights.third(1)])
        on_step(t, 15, [lambda: weights.third(2)])
        depth = window(near_depth(pick(t, dzs), pick(t, dus)) * 256, 256)
        proj[0:384, :] += dot(tbuf[0:384, depth], wbuf[depth, :])

    def opiece(dz, du, part, sub):
        cols = window(lax.rem(z + (dz + 4), 4) * 256, 256)
        start, size = ((0, 64), (64, 192))[part]
        base = lax.rem(u + (du + 4), 4) * 256 + start
        if sub is None:
            return obuf.at[pl.ds(pl.multiple_of(base, 64), size), cols]
        return obuf.at[pl.ds(pl.multiple_of(base + sub * (size // 2), 32), size // 2), cols]

    for c in (0, 1):
        links.arrived(obuf.at[window(u * 256, 256), window(z * 256 + c * 128, 128)], sss.at[5], srs.at[c * 6 + 5])
    columns = TorusGather(links, opiece, oss, ors, obuf.at[pl.ds(0, 960), :])
    columns.begin()

    def turned(i, rows):
        v = proj[rows, i * QK : (i + 1) * QK]
        swapped = jnp.concatenate([v[:, QK // 2 :], v[:, : QK // 2]], axis=1)
        return (v * cos[rows] + swapped * sin[rows]).astype(BF)

    def keep_keys(start, size):
        rows = slice(start, start + size)
        at = pl.ds(pl.multiple_of(place * ROWS + start, 128), size)
        kvbuf[at, 0:QK] = turned(2, rows)
        kvbuf[at, QK : 2 * QK] = turned(3, rows)
        kvbuf[at, 2 * QK :] = proj[rows, 4 * QK :].astype(BF)

    keep_keys(0, 384)
    far_tokens()
    proj[384:512, 2 * QK :] = dot(tbuf[384:512, :], wbuf[:, 2 * QK :])
    keep_keys(384, 128)

    def kpiece(dz, du, part, sub):
        start, size = ((0, 128), (128, 384))[part]
        base = slot(dz, du) * ROWS + start
        if sub is None:
            return kvbuf.at[pl.ds(pl.multiple_of(base, 128), size), :]
        return kvbuf.at[pl.ds(pl.multiple_of(base + sub * (size // 2), 64), size // 2), :]

    keys = TorusGather(links, kpiece, kss, krs, kvbuf.at[pl.ds(0, 7680), :])
    keys.begin()
    crosses = jnp.logical_and(core == 1, crossed)
    plain(lown, lrecv, xss.at[0], xrs.at[0], "odd", only=crosses)
    pl.when(jnp.logical_not(crosses))(lambda: pltpu.make_async_copy(lown, lrecv, xrs.at[0]).start())
    proj[384:512, 0 : 2 * QK] = dot(tbuf[384:512, :], wbuf[:, 0 : 2 * QK])
    qbuf[0] = turned(0, slice(0, ROWS))
    qbuf[1] = turned(1, slice(0, ROWS))

    def attend(index, at_u, masked, opening):
        span = window(index * ROWS, ROWS)
        v = kvbuf[span, 2 * QK :]
        for r in range(2):
            rows = pl.ds(r * 256, 256)
            if masked:
                query_at = positions(r * 256 + lax.broadcasted_iota(jnp.int32, (256, ROWS), 0), u)
                key_at = positions(lax.broadcasted_iota(jnp.int32, (256, ROWS), 1), at_u)
                allowed = key_at <= query_at
            for a in range(2):
                s = dot(qbuf[a, rows], kvbuf[span, a * QK : (a + 1) * QK], (((1,), (1,)), ((), ())))
                if masked:
                    s = jnp.where(allowed, s, -1e30)
                parts = [s[:, k * 128 : (k + 1) * 128] for k in range(4)]
                high = jnp.maximum(jnp.maximum(parts[0], parts[1]), jnp.maximum(parts[2], parts[3]))
                high = jnp.max(high, axis=1, keepdims=True) * log_scale
                if opening:
                    new = high
                else:
                    old = top[a, rows][:, :1]
                    new = jnp.maximum(old, high)
                e = jnp.exp2(s * log_scale - new)
                total = (e[:, 0:128] + e[:, 128:256]) + (e[:, 256:384] + e[:, 384:512])
                weighted = dot(e.astype(BF), v)
                if opening:
                    tot[a, rows] = total
                    acc[a, rows] = weighted
                else:
                    fade = jnp.exp2(old - new)
                    tot[a, rows] = tot[a, rows] * fade + total
                    acc[a, rows] = acc[a, rows] * fade + weighted
                top[a, rows] = jnp.broadcast_to(new, (256, 128))

    attend(place, u, True, True)

    ksteps = keys.steps()
    csteps = columns.steps()
    early_columns = [[] for _ in range(15)]
    for k in range(15):
        early_columns[max(k - 1, 0)] += csteps[k][0]

    @pl.loop(0, 15)
    def _(t):
        for k in range(15):
            on_step(t, k, early_columns[k] + ksteps[k][0])
        at_z = lax.rem(z + pick(t, dzs[1:]) + 4, 4)
        at_u = lax.rem(u + pick(t, dus[1:]) + 4, 4)
        index = at_z * 4 + at_u
        before = jnp.logical_and(at_z == z, jnp.logical_and(core == 0, at_u < u))

        @pl.when(jnp.logical_or(at_z < z, before))
        def _():
            attend(index, at_u, False, False)

        @pl.when(jnp.logical_and(at_z == z, core == 1))
        def _():
            attend(index, at_u, True, False)

    links.arrived(lrecv, xss.at[0], xrs.at[0])

    def finish(h):
        rows = pl.ds(h * 256, 256)
        o1 = acc[0, rows] / jnp.sum(tot[0, rows], axis=1, keepdims=True)
        o2 = acc[1, rows] / jnp.sum(tot[1, rows], axis=1, keepdims=True)
        mixed = o1 - lrecv[0:1, 0:1] * o2
        norm = lax.rsqrt(jnp.mean(mixed * mixed, axis=1, keepdims=True) + EPS_NORM)
        abuf[0, rows] = (mixed * norm * gain[...]).astype(BF)

    def heads(k, h):
        return abuf.at[k, pl.ds(h * 256, 256), :]

    def along(src, dst, k, step):
        plain(src, dst, xss.at[k], xrs.at[k], "w", step)

    def got(view, k):
        links.arrived(view, xss.at[k], xrs.at[k])

    seen = set()

    def add(dw, h):
        head = window(lax.rem(w + (dw + 4), 4) * 256, 256)
        term = dot(abuf[NEAR.index(dw), h * 256 : (h + 1) * 256, :], obuf[head, :])
        for b in (0, 1):
            target = (dw + NEAR[2 * h + b]) % 4
            j = NEAR.index(-1 if target == 3 else target)
            block = term[b * 128 : (b + 1) * 128]
            if j in seen:
                osum[j] += block
            else:
                osum[j] = block
            seen.add(j)

    finish(0)
    along(heads(0, 0), heads(1, 0), 1, 1)
    finish(1)
    along(heads(0, 1), heads(2, 1), 4, -1)
    along(heads(0, 0), heads(2, 0), 3, -1)
    along(heads(0, 1), heads(1, 1), 2, 1)
    add(0, 0)
    add(0, 1)
    got(heads(1, 0), 1)
    along(heads(1, 0), heads(3, 0), 5, 1)
    got(heads(2, 1), 4)
    along(heads(2, 1), heads(3, 1), 6, -1)
    add(-1, 0)
    add(1, 1)
    got(heads(1, 1), 2)
    add(-1, 1)
    got(heads(2, 0), 3)
    add(1, 0)
    got(heads(3, 0), 5)
    add(2, 0)
    got(heads(3, 1), 6)
    add(2, 1)

    for r, step in ((0, 1), (1, -1)):
        fsend[r] = osum[3, r * 64 : (r + 1) * 64].astype(BF)
        along(fsend.at[r], passing.at[r], 7 + r, step)
    nsend[0] = osum[2].astype(BF)
    along(nsend.at[0], fin.at[1], 9, 1)
    nsend[1] = osum[1].astype(BF)
    along(nsend.at[1], fin.at[2], 10, -1)
    fin[0] = osum[0].astype(BF)
    other_rows = window(other * 64, 64)

    def to_sibling(k):
        at_w = lax.rem(w + (NEAR[k] + 4), 4)
        plain(fin.at[k, other_rows, :], sib.at[at_w], xss.at[13 + k], xrs.at[13 + at_w], "core")

    to_sibling(0)
    for r, step in ((0, 1), (1, -1)):
        got(passing.at[r], 7 + r)
        along(passing.at[r], fin.at[3, pl.ds(r * 64, 64), :], 11 + r, step)
    got(fin.at[1], 9)
    to_sibling(1)
    got(fin.at[2], 10)
    to_sibling(2)
    got(fin.at[3, pl.ds(0, 64), :], 11)
    got(fin.at[3, pl.ds(64, 64), :], 12)
    to_sibling(3)
    own_part = window(core * 64, 64)
    for k in range(4):
        at_w = lax.rem(w + (NEAR[k] + 4), 4)
        links.arrived(sib.at[at_w], xss.at[13 + k], xrs.at[13 + at_w])
        both = (fin[k, own_part, :].astype(F32) + sib[at_w].astype(F32)).astype(BF)
        for c in range(4):
            out[:, window((c * 4 + at_w) * 256, 256)] = both[:, c * 256 : (c + 1) * 256]
    links.drain()


def on_device(tokens, query_one, query_two, key_one, key_two, value_weight, out_weight, lambdas, head_gain):
    inverse = 1.0 / np.float32(ROPE_BASE) ** (np.arange(0, QK, 2, dtype=np.float32) / np.float32(QK))
    vm = pl.BlockSpec(memory_space=pltpu.VMEM)
    dma = pltpu.SemaphoreType.DMA
    return pl.pallas_call(
        layer_kernel,
        out_shape=jax.ShapeDtypeStruct((64, 4096), BF),
        in_specs=[vm] * 7 + [pl.BlockSpec(memory_space=pltpu.SMEM)] + [vm] * 2,
        out_specs=vm,
        scratch_shapes=[
            pltpu.VMEM((ROWS, QK), F32),
            pltpu.VMEM((ROWS, QK), F32),
            pltpu.VMEM((ROWS, 4096), BF),
            pltpu.VMEM((4096, 768), BF),
            pltpu.VMEM((ROWS, 768), F32),
            pltpu.VMEM((2, ROWS, QK), BF),
            pltpu.VMEM((8192, 512), BF),
            pltpu.VMEM((1024, 1024), BF),
            pltpu.VMEM((2, ROWS, V), F32),
            pltpu.VMEM((2, ROWS, 128), F32),
            pltpu.VMEM((2, ROWS, 128), F32),
            pltpu.VMEM((4, ROWS, V), BF),
            pltpu.VMEM((4, 128, 1024), F32),
            pltpu.VMEM((2, 64, 1024), BF),
            pltpu.VMEM((2, 64, 1024), BF),
            pltpu.VMEM((2, 128, 1024), BF),
            pltpu.VMEM((4, 128, 1024), BF),
            pltpu.VMEM((4, 64, 1024), BF),
            pltpu.VMEM((8, 128), F32),
            pltpu.VMEM((8, 128), F32),
            dma((1,)),
            dma((1,)), dma((40,)),
            dma((1,)), dma((40,)),
            dma((1,)), dma((40,)),
            dma((7,)), dma((7,)),
            dma((12,)), dma((12,)),
            dma((17,)), dma((17,)),
        ],
        compiler_params=pltpu.CompilerParams(
            collective_id=0, has_side_effects=True, vmem_limit_bytes=62 * 1024 * 1024
        ),
    )(tokens, query_one, query_two, key_one, key_two, value_weight, out_weight, lambdas, head_gain[None], jnp.asarray(inverse[None], F32))


def solution(mesh):
    fine = Mesh(mesh.devices.reshape(4, 4, 2, 4), AXES)
    sp = ("z", "y", "core")
    in_specs = (
        P((*sp, "x"), None),
        P(sp, "x"),
        P(sp, "x"),
        P(sp, "x"),
        P(sp, "x"),
        P(sp, "x"),
        P("x", sp),
        P("x"),
        P(),
    )
    return jax.shard_map(on_device, mesh=fine, in_specs=in_specs, out_specs=P((*sp, "x"), None), check_vma=False)
```

```python
import jax
import jax.numpy as jnp
import numpy as np
from jax import lax
from jax.experimental import pallas as pl
from jax.experimental.pallas import tpu as pltpu
from jax.sharding import Mesh, PartitionSpec as P

QK = 128
V = 256
ROPE_BASE = 500000.0
EPS_NORM = 0.02
LOG2E = 1.4426950408889634
ROWS = 512
BF = jnp.bfloat16
F32 = jnp.float32
MESH = pl.DeviceIdType.MESH
AXES = ("z", "y", "core", "x")
NEAR = (0, -1, 1, 2)


def dot(a, b, dims=(((1,), (0,)), ((), ()))):
    return lax.dot_general(a, b, dims, preferred_element_type=F32)


class Links:
    def __init__(self):
        self.z, self.y, self.core, self.x = [lax.axis_index(a) for a in AXES]
        self.u = self.y * (1 - self.core) + self.x * self.core
        self.w = self.x * (1 - self.core) + self.y * self.core
        self.sent = []
        self.later = []

    def peer(self, axis, step):
        if axis == "core":
            return {"core": 1 - self.core}
        if axis == "even":
            return {"core": 0}
        if axis == "turned":
            return {"y": self.x, "core": 0, "x": self.y}
        if axis == "odd":
            return {"y": self.x, "core": 1, "x": lax.rem(2 * self.x - self.y + 4, 4)}
        if axis == "z":
            return {"z": lax.rem(self.z + (step + 4), 4)}
        along = self.core if axis == "u" else 1 - self.core
        return {"y": lax.rem(self.y + (4 + step * (1 - along)), 4), "x": lax.rem(self.x + (4 + step * along), 4)}

    def send(self, views, axis, step, only=None, noted=True):
        def copy():
            return pltpu.make_async_remote_copy(*views(), device_id=self.peer(axis, step), device_id_type=MESH)

        if only is None:
            copy().start()
        else:
            pl.when(only)(lambda: copy().start())
        if noted:
            self.sent.append((copy, only))

    def arrived(self, view, ssem, rsem):
        pltpu.make_async_remote_copy(view, view, ssem, rsem, device_id=self.peer("core", 1), device_id_type=MESH).wait_recv()

    def drain(self):
        for copy, only in self.sent:
            if only is None:
                copy().wait_send()
            else:
                pl.when(only)(lambda copy=copy: copy().wait_send())
        for view, ssem in self.later:
            pltpu.make_async_remote_copy(view, view, ssem, ssem, device_id=self.peer("core", 1), device_id_type=MESH).wait_send()


class TorusGather:
    def __init__(self, links, piece, ssem, rsem, all_sent):
        self.links, self.piece, self.ssem, self.rsem = links, piece, ssem, rsem
        links.later.append((all_sent, ssem.at[0]))

    def ref(self, part, dp, ds, sub=None):
        dz, du = (ds, dp) if part == 0 else (dp, ds)
        return self.piece(dz, du, part, sub)

    def axis(self, part, second):
        return ("u", "z")[part ^ second]

    def out(self, part, key, dp, ds, sub, second, step):
        k = part * 15 + key

        def views():
            view = self.ref(part, dp, ds, sub)
            return view, view, self.ssem.at[0], self.rsem.at[k]

        self.links.send(views, self.axis(part, second), step, noted=False)

    def wait(self, part, key, dp, ds, sub):
        k = part * 15 + key
        self.links.arrived(self.ref(part, dp, ds, sub), self.ssem.at[0], self.rsem.at[k])

    def spread(self, part, dp):
        i = NEAR.index(dp)
        self.out(part, 3 + 3 * i, dp, 0, None, 1, 1)
        self.out(part, 4 + 3 * i, dp, 0, None, 1, -1)

    def begin(self):
        for part in (0, 1):
            self.out(part, 0, 0, 0, None, 0, 1)
            self.out(part, 1, 0, 0, None, 0, -1)
        for part in (0, 1):
            self.spread(part, 0)

    def first(self):
        for part in (0, 1):
            self.wait(part, 0, -1, 0, None)
            self.out(part, 2, -1, 0, 0, 0, 1)
            self.wait(part, 1, 1, 0, None)
            self.out(part, 2, 1, 0, 1, 0, -1)
        for part in (0, 1):
            self.spread(part, -1)
            self.spread(part, 1)

    def opposite(self):
        for part in (0, 1):
            self.wait(part, 2, 2, 0, None)
            self.spread(part, 2)

    def second(self, dp, step):
        i = NEAR.index(dp)
        for part in (0, 1):
            if step < 0:
                self.wait(part, 3 + 3 * i, dp, -1, None)
                self.out(part, 5 + 3 * i, dp, -1, 0, 1, 1)
            else:
                self.wait(part, 4 + 3 * i, dp, 1, None)
                self.out(part, 5 + 3 * i, dp, 1, 1, 1, -1)

    def third(self, dp):
        i = NEAR.index(dp)
        for part in (0, 1):
            self.wait(part, 5 + 3 * i, dp, 2, None)

    def steps(self):
        second, third = self.second, self.third
        return [
            ([self.first, lambda: second(0, -1)], (-1, 0)),
            ([], (0, -1)),
            ([lambda: second(0, 1)], (1, 0)),
            ([], (0, 1)),
            ([self.opposite, lambda: second(-1, -1)], (-1, -1)),
            ([lambda: second(-1, 1), lambda: second(1, -1)], (1, -1)),
            ([], (-1, 1)),
            ([lambda: second(1, 1)], (1, 1)),
            ([lambda: third(0)], (0, 2)),
            ([], (2, 0)),
            ([lambda: second(2, -1), lambda: second(2, 1), lambda: third(-1)], (-1, 2)),
            ([], (2, -1)),
            ([lambda: third(1)], (1, 2)),
            ([], (2, 1)),
            ([lambda: third(2)], (2, 2)),
        ]


def pick(t, values):
    result = values[0]
    for k in range(1, len(values)):
        result = jnp.where(t == k, values[k], result)
    return result


def on_step(t, k, actions):
    if actions:

        @pl.when(t == k)
        def _():
            for action in actions:
                action()


def window(start, size):
    return pl.ds(pl.multiple_of(start, size), size)


def layer_kernel(
    tok, wq1, wq2, wk1, wk2, wv, wo, lam, gain, inverse, out, cos, sin,
    tbuf, wbuf, proj, qbuf, kvbuf, obuf, acc, top, tot,
    abuf, osum, fsend, passing, nsend, fin, sib, lown, lrecv,
    lsem, wss, wrs, kss, krs, oss, ors, tss, trs, sss, srs, xss, xrs,
):
    links = Links()
    z, y, core, x, u, w = links.z, links.y, links.core, links.x, links.u, links.w
    other = 1 - core
    chip = z * 4 + y
    place = z * 4 + u
    log_scale = QK ** (-0.5) * LOG2E

    def slot(dz, du):
        return lax.rem(z + (dz + 4), 4) * 4 + lax.rem(u + (du + 4), 4)

    def depth_of(at_z, at_u):
        return at_z * 4 + jnp.where(core == 0, at_u, lax.rem(2 * w - at_u + 4, 4))

    def near_depth(dz, du):
        return depth_of(lax.rem(z + (dz + 4), 4), lax.rem(u + (du + 4), 4))

    own_depth = depth_of(z, u)

    def plain(src, dst, ssem, rsem, axis, step=1, only=None):
        links.send(lambda: (src, dst, ssem, rsem), axis, step, only)

    barrier = pltpu.get_barrier_semaphore()
    for axis, step in [("core", 1)] + [(a, s) for a in ("u", "w", "z") for s in (1, -1)]:
        pl.semaphore_signal(barrier, inc=1, device_id=links.peer(axis, step), device_id_type=MESH)
    crossed = x != y

    @pl.when(jnp.logical_and(core == 1, crossed))
    def _():
        for c in (0, 1):
            source = {"y": lax.rem(2 * y - x + 4, 4), "core": c, "x": y}
            pl.semaphore_signal(barrier, inc=1, device_id=source, device_id_type=MESH)

    @pl.when(jnp.logical_and(core == 0, crossed))
    def _():
        for c in (0, 1):
            pl.semaphore_signal(barrier, inc=1, device_id={"y": x, "core": c, "x": y}, device_id_type=MESH)

    pl.semaphore_wait(barrier, 7 + jnp.where(crossed, 2, 0))

    def trows(dw, c):
        return tbuf.at[window(NEAR.index(dw) * 128 + c * 64, 64), :]

    own_tokens = pltpu.make_async_copy(tok, trows(0, core), lsem.at[0])
    own_tokens.start()

    own_rows = window(chip * 256 + core * 128, 128)
    items = []
    column = 0
    for ref, width in ((wq1, QK), (wq2, QK), (wk1, QK), (wk2, QK), (wv, V)):
        cols = pl.ds(column, width)
        items.append((ref.at[:, pl.ds(0, width)], ref.at[:, pl.ds(width, width)], wbuf.at[own_rows, cols]))
        column += width
    stays = jnp.logical_and(core == 1, x == y)
    leaves = jnp.logical_not(stays)

    def hand_over(which):
        for i in which:
            even, odd, dst = items[i]
            k = core * 6 + i
            plain(odd, dst, sss.at[6 + i], srs.at[k], "odd", only=leaves)
            pl.when(stays)(lambda: pltpu.make_async_copy(odd, dst, srs.at[k]).start())
            plain(even, dst, sss.at[i], srs.at[k], "even", only=core == 1)
            pl.when(core == 0)(lambda: pltpu.make_async_copy(even, dst, srs.at[k]).start())

    def hand_over_out():
        dst = obuf.at[window(x * 256, 256), window(z * 256 + core * 128, 128)]
        even, odd = wo.at[pl.ds(0, 256), :], wo.at[pl.ds(256, 256), :]
        k = core * 6 + 5
        here = jnp.logical_and(core == 0, x == y)
        plain(even, dst, sss.at[5], srs.at[k], "turned", only=jnp.logical_not(here))
        pl.when(here)(lambda: pltpu.make_async_copy(even, dst, srs.at[k]).start())
        plain(odd, dst, sss.at[11], srs.at[k], "core", only=core == 0)
        pl.when(core == 1)(lambda: pltpu.make_async_copy(odd, dst, srs.at[k]).start())

    hand_over(range(5))
    plain(tok, tbuf.at[window(core * 64, 64), :], tss.at[6], trs.at[6], "core")
    plain(tok, tbuf.at[window(NEAR.index(-1) * 128 + core * 64, 64), :], tss.at[core], trs.at[core], "w", 1)
    hand_over_out()

    for c in (0, 1):
        column = 0
        for i, width in enumerate((QK, QK, QK, QK, V)):
            view = wbuf.at[window(own_depth * 256 + c * 128, 128), pl.ds(column, width)]
            links.arrived(view, sss.at[i], srs.at[c * 6 + i])
            column += width

    def wpiece(dz, du, part, sub):
        start = near_depth(dz, du) * 256 + part * 128
        if sub is None:
            return wbuf.at[window(start, 128), :]
        return wbuf.at[window(start + sub * 64, 64), :]

    weights = TorusGather(links, wpiece, wss, wrs, wbuf.at[pl.ds(0, 3840), :])
    weights.begin()

    links.arrived(trows(0, other), tss.at[6], trs.at[6])
    sibling = trows(0, other)
    plain(sibling, tbuf.at[window(NEAR.index(1) * 128 + other * 64, 64), :], tss.at[2 + other], trs.at[2 + other], "w", -1)
    plain(tok, tbuf.at[window(NEAR.index(1) * 128 + core * 64, 64), :], tss.at[2 + core], trs.at[2 + core], "w", -1)
    plain(sibling, tbuf.at[window(NEAR.index(-1) * 128 + other * 64, 64), :], tss.at[other], trs.at[other], "w", 1)

    lown[...] = jnp.full((8, 128), jnp.where(core == 0, lam[0], lam[1]), F32)

    def pass_on(dw, c, k, step):
        links.send(lambda: (trows(dw, c), trows(2, c), tss.at[k], trs.at[k]), "w", step)

    def near_tokens():
        links.arrived(trows(-1, core), tss.at[core], trs.at[core])
        pass_on(-1, core, 4, 1)
        links.arrived(trows(1, other), tss.at[2 + other], trs.at[2 + other])
        pass_on(1, other, 5, -1)

    def near_tokens_rest():
        links.arrived(trows(-1, other), tss.at[other], trs.at[other])
        links.arrived(trows(1, core), tss.at[2 + core], trs.at[2 + core])
        own_tokens.wait()

    def far_tokens():
        links.arrived(trows(2, core), tss.at[4], trs.at[4])
        links.arrived(trows(2, other), tss.at[5], trs.at[5])

    def positions(ids, at_u):
        rel = ids // 128
        step = jnp.where(rel == 1, 3, jnp.where(rel == 2, 1, jnp.where(rel == 3, 2, 0)))
        along = (w + step) & 3
        return z * 2048 + at_u * (512 - 448 * core) + along * (64 + 448 * core) + ((ids // 64) & 1) * 256 + (ids & 63)

    half_dim = QK // 2
    position = positions(lax.broadcasted_iota(jnp.int32, (ROWS, half_dim), 0), u)
    angle = position.astype(F32) * inverse[...]
    cos_part, sin_part = jnp.cos(angle), jnp.sin(angle)
    cos[:, :half_dim] = cos_part
    cos[:, half_dim:] = cos_part
    sin[:, :half_dim] = -sin_part
    sin[:, half_dim:] = sin_part
    proj[...] = jnp.zeros_like(proj)

    steps = weights.steps()
    early = [action for actions, _ in steps[:6] for action in actions] + [near_tokens]
    early += [action for actions, _ in steps[6:8] for action in actions] + [near_tokens_rest]
    dzs = [0] + [d for _, (d, _) in steps]
    dus = [0] + [d for _, (_, d) in steps]

    @pl.loop(0, 16)
    def _(t):
        on_step(t, 0, early)
        on_step(t, 5, [lambda: weights.third(0), lambda: weights.second(2, -1), lambda: weights.second(2, 1)])
        on_step(t, 11, [lambda: weights.third(-1)])
        on_step(t, 13, [lambda: weights.third(1)])
        on_step(t, 15, [lambda: weights.third(2)])
        depth = window(near_depth(pick(t, dzs), pick(t, dus)) * 256, 256)
        proj[0:384, :] += dot(tbuf[0:384, depth], wbuf[depth, :])

    def opiece(dz, du, part, sub):
        cols = window(lax.rem(z + (dz + 4), 4) * 256, 256)
        start, size = ((0, 64), (64, 192))[part]
        base = lax.rem(u + (du + 4), 4) * 256 + start
        if sub is None:
            return obuf.at[pl.ds(pl.multiple_of(base, 64), size), cols]
        return obuf.at[pl.ds(pl.multiple_of(base + sub * (size // 2), 32), size // 2), cols]

    for c in (0, 1):
        links.arrived(obuf.at[window(u * 256, 256), window(z * 256 + c * 128, 128)], sss.at[5], srs.at[c * 6 + 5])
    columns = TorusGather(links, opiece, oss, ors, obuf.at[pl.ds(0, 960), :])
    columns.begin()

    def turned(i, rows):
        v = proj[rows, i * QK : (i + 1) * QK]
        swapped = jnp.concatenate([v[:, QK // 2 :], v[:, : QK // 2]], axis=1)
        return (v * cos[rows] + swapped * sin[rows]).astype(BF)

    def keep_keys(start, size):
        rows = slice(start, start + size)
        at = pl.ds(pl.multiple_of(place * ROWS + start, 128), size)
        kvbuf[at, 0:QK] = turned(2, rows)
        kvbuf[at, QK : 2 * QK] = turned(3, rows)
        kvbuf[at, 2 * QK :] = proj[rows, 4 * QK :].astype(BF)

    keep_keys(0, 384)
    far_tokens()
    proj[384:512, 2 * QK :] = dot(tbuf[384:512, :], wbuf[:, 2 * QK :])
    keep_keys(384, 128)

    def kpiece(dz, du, part, sub):
        start, size = ((0, 128), (128, 384))[part]
        base = slot(dz, du) * ROWS + start
        if sub is None:
            return kvbuf.at[pl.ds(pl.multiple_of(base, 128), size), :]
        return kvbuf.at[pl.ds(pl.multiple_of(base + sub * (size // 2), 64), size // 2), :]

    keys = TorusGather(links, kpiece, kss, krs, kvbuf.at[pl.ds(0, 7680), :])
    keys.begin()
    crosses = jnp.logical_and(core == 1, crossed)
    plain(lown, lrecv, xss.at[0], xrs.at[0], "odd", only=crosses)
    pl.when(jnp.logical_not(crosses))(lambda: pltpu.make_async_copy(lown, lrecv, xrs.at[0]).start())
    proj[384:512, 0 : 2 * QK] = dot(tbuf[384:512, :], wbuf[:, 0 : 2 * QK])
    qbuf[0] = turned(0, slice(0, ROWS))
    qbuf[1] = turned(1, slice(0, ROWS))

    def attend(index, at_u, masked, opening):
        span = window(index * ROWS, ROWS)
        v = kvbuf[span, 2 * QK :]
        for r in range(2):
            rows = pl.ds(r * 256, 256)
            if masked:
                query_at = positions(r * 256 + lax.broadcasted_iota(jnp.int32, (256, ROWS), 0), u)
                key_at = positions(lax.broadcasted_iota(jnp.int32, (256, ROWS), 1), at_u)
                allowed = key_at <= query_at
            for a in range(2):
                s = dot(qbuf[a, rows], kvbuf[span, a * QK : (a + 1) * QK], (((1,), (1,)), ((), ())))
                if masked:
                    s = jnp.where(allowed, s, -1e30)
                parts = [s[:, k * 128 : (k + 1) * 128] for k in range(4)]
                high = jnp.maximum(jnp.maximum(parts[0], parts[1]), jnp.maximum(parts[2], parts[3]))
                high = jnp.max(high, axis=1, keepdims=True) * log_scale
                if opening:
                    new = high
                else:
                    old = top[a, rows][:, :1]
                    new = jnp.maximum(old, high)
                e = jnp.exp2(s * log_scale - new)
                total = (e[:, 0:128] + e[:, 128:256]) + (e[:, 256:384] + e[:, 384:512])
                weighted = dot(e.astype(BF), v)
                if opening:
                    tot[a, rows] = total
                    acc[a, rows] = weighted
                else:
                    fade = jnp.exp2(old - new)
                    tot[a, rows] = tot[a, rows] * fade + total
                    acc[a, rows] = acc[a, rows] * fade + weighted
                top[a, rows] = jnp.broadcast_to(new, (256, 128))

    attend(place, u, True, True)

    ksteps = keys.steps()
    csteps = columns.steps()
    early_columns = [[] for _ in range(15)]
    for k in range(15):
        early_columns[max(k - 1, 0)] += csteps[k][0]

    @pl.loop(0, 15)
    def _(t):
        for k in range(15):
            on_step(t, k, early_columns[k] + ksteps[k][0])
        at_z = lax.rem(z + pick(t, dzs[1:]) + 4, 4)
        at_u = lax.rem(u + pick(t, dus[1:]) + 4, 4)
        index = at_z * 4 + at_u
        before = jnp.logical_and(at_z == z, jnp.logical_and(core == 0, at_u < u))

        @pl.when(jnp.logical_or(at_z < z, before))
        def _():
            attend(index, at_u, False, False)

        @pl.when(jnp.logical_and(at_z == z, core == 1))
        def _():
            attend(index, at_u, True, False)

    links.arrived(lrecv, xss.at[0], xrs.at[0])

    def finish(h):
        rows = pl.ds(h * 256, 256)
        o1 = acc[0, rows] / jnp.sum(tot[0, rows], axis=1, keepdims=True)
        o2 = acc[1, rows] / jnp.sum(tot[1, rows], axis=1, keepdims=True)
        mixed = o1 - lrecv[0:1, 0:1] * o2
        norm = lax.rsqrt(jnp.mean(mixed * mixed, axis=1, keepdims=True) + EPS_NORM)
        abuf[0, rows] = (mixed * norm * gain[...]).astype(BF)

    def heads(k, h):
        return abuf.at[k, pl.ds(h * 256, 256), :]

    def along(src, dst, k, step):
        plain(src, dst, xss.at[k], xrs.at[k], "w", step)

    def got(view, k):
        links.arrived(view, xss.at[k], xrs.at[k])

    seen = set()

    def add(dw, h):
        head = window(lax.rem(w + (dw + 4), 4) * 256, 256)
        term = dot(abuf[NEAR.index(dw), h * 256 : (h + 1) * 256, :], obuf[head, :])
        for b in (0, 1):
            target = (dw + NEAR[2 * h + b]) % 4
            j = NEAR.index(-1 if target == 3 else target)
            block = term[b * 128 : (b + 1) * 128]
            if j in seen:
                osum[j] += block
            else:
                osum[j] = block
            seen.add(j)

    finish(0)
    along(heads(0, 0), heads(1, 0), 1, 1)
    finish(1)
    along(heads(0, 1), heads(2, 1), 4, -1)
    along(heads(0, 0), heads(2, 0), 3, -1)
    along(heads(0, 1), heads(1, 1), 2, 1)
    add(0, 0)
    add(0, 1)
    got(heads(1, 0), 1)
    along(heads(1, 0), heads(3, 0), 5, 1)
    got(heads(2, 1), 4)
    along(heads(2, 1), heads(3, 1), 6, -1)
    add(-1, 0)
    add(1, 1)
    got(heads(1, 1), 2)
    add(-1, 1)
    got(heads(2, 0), 3)
    add(1, 0)
    got(heads(3, 0), 5)
    add(2, 0)
    got(heads(3, 1), 6)
    add(2, 1)

    for r, step in ((0, 1), (1, -1)):
        fsend[r] = osum[3, r * 64 : (r + 1) * 64].astype(BF)
        along(fsend.at[r], passing.at[r], 7 + r, step)
    nsend[0] = osum[2].astype(BF)
    along(nsend.at[0], fin.at[1], 9, 1)
    nsend[1] = osum[1].astype(BF)
    along(nsend.at[1], fin.at[2], 10, -1)
    fin[0] = osum[0].astype(BF)
    other_rows = window(other * 64, 64)

    def to_sibling(k):
        at_w = lax.rem(w + (NEAR[k] + 4), 4)
        plain(fin.at[k, other_rows, :], sib.at[at_w], xss.at[13 + k], xrs.at[13 + at_w], "core")

    to_sibling(0)
    for r, step in ((0, 1), (1, -1)):
        got(passing.at[r], 7 + r)
        along(passing.at[r], fin.at[3, pl.ds(r * 64, 64), :], 11 + r, step)
    got(fin.at[1], 9)
    to_sibling(1)
    got(fin.at[2], 10)
    to_sibling(2)
    got(fin.at[3, pl.ds(0, 64), :], 11)
    got(fin.at[3, pl.ds(64, 64), :], 12)
    to_sibling(3)
    own_part = window(core * 64, 64)
    for k in range(4):
        at_w = lax.rem(w + (NEAR[k] + 4), 4)
        links.arrived(sib.at[at_w], xss.at[13 + k], xrs.at[13 + at_w])
        both = (fin[k, own_part, :].astype(F32) + sib[at_w].astype(F32)).astype(BF)
        for c in range(4):
            out[:, window((c * 4 + at_w) * 256, 256)] = both[:, c * 256 : (c + 1) * 256]
    links.drain()


def on_device(tokens, query_one, query_two, key_one, key_two, value_weight, out_weight, lambdas, head_gain):
    inverse = 1.0 / np.float32(ROPE_BASE) ** (np.arange(0, QK, 2, dtype=np.float32) / np.float32(QK))
    vm = pl.BlockSpec(memory_space=pltpu.VMEM)
    dma = pltpu.SemaphoreType.DMA
    return pl.pallas_call(
        layer_kernel,
        out_shape=jax.ShapeDtypeStruct((64, 4096), BF),
        in_specs=[vm] * 7 + [pl.BlockSpec(memory_space=pltpu.SMEM)] + [vm] * 2,
        out_specs=vm,
        scratch_shapes=[
            pltpu.VMEM((ROWS, QK), F32),
            pltpu.VMEM((ROWS, QK), F32),
            pltpu.VMEM((ROWS, 4096), BF),
            pltpu.VMEM((4096, 768), BF),
            pltpu.VMEM((ROWS, 768), F32),
            pltpu.VMEM((2, ROWS, QK), BF),
            pltpu.VMEM((8192, 512), BF),
            pltpu.VMEM((1024, 1024), BF),
            pltpu.VMEM((2, ROWS, V), F32),
            pltpu.VMEM((2, ROWS, 128), F32),
            pltpu.VMEM((2, ROWS, 128), F32),
            pltpu.VMEM((4, ROWS, V), BF),
            pltpu.VMEM((4, 128, 1024), F32),
            pltpu.VMEM((2, 64, 1024), BF),
            pltpu.VMEM((2, 64, 1024), BF),
            pltpu.VMEM((2, 128, 1024), BF),
            pltpu.VMEM((4, 128, 1024), BF),
            pltpu.VMEM((4, 64, 1024), BF),
            pltpu.VMEM((8, 128), F32),
            pltpu.VMEM((8, 128), F32),
            dma((1,)),
            dma((1,)), dma((30,)),
            dma((1,)), dma((30,)),
            dma((1,)), dma((30,)),
            dma((7,)), dma((7,)),
            dma((12,)), dma((12,)),
            dma((17,)), dma((17,)),
        ],
        compiler_params=pltpu.CompilerParams(
            collective_id=0, has_side_effects=True, vmem_limit_bytes=62 * 1024 * 1024
        ),
    )(tokens, query_one, query_two, key_one, key_two, value_weight, out_weight, lambdas, head_gain[None], jnp.asarray(inverse[None], F32))


def solution(mesh):
    fine = Mesh(mesh.devices.reshape(4, 4, 2, 4), AXES)
    sp = ("z", "y", "core")
    in_specs = (
        P((*sp, "x"), None),
        P(sp, "x"),
        P(sp, "x"),
        P(sp, "x"),
        P(sp, "x"),
        P(sp, "x"),
        P("x", sp),
        P("x"),
        P(),
    )
    return jax.shard_map(on_device, mesh=fine, in_specs=in_specs, out_specs=P((*sp, "x"), None), check_vma=False)
```
